32 devices in a mesh: fs: 8 (over z, y), tp: 4 (over x, core).
Axes of the slice: x: 2, y: 2, z: 4, core: 2. Of those that a mesh axis runs over, the one named last changes fastest.
Arguments:
- resid: bfloat16 [8192, 2048], P(('fs', 'tp')), may hold values from -6 to 6
- mix_gain: float32 [2048], replicated, may hold values from 0.1 to 1.9
- w_query: bfloat16 [2048, 1024], P('fs', 'tp'), may hold values from -0.125 to 0.125
- w_key: bfloat16 [2048, 1024], P('fs', 'tp'), may hold values from -0.125 to 0.125
- w_value: bfloat16 [2048, 2048], P('fs', 'tp'), may hold values from -0.125 to 0.125
- w_gate: bfloat16 [2048, 2048], P('fs', 'tp'), may hold values from -0.125 to 0.125
- w_output: bfloat16 [2048, 2048], P('tp', 'fs'), may hold values from -0.125 to 0.125
- decay_rate: float32 [8], P('tp'), may hold values from 0.0008 to 0.034, as said below
- mlp_gain: float32 [2048], replicated, may hold values from 0.1 to 1.9
- w_up: bfloat16 [2048, 8192], P('fs', 'tp'), may hold values from -0.125 to 0.125
- w_down: bfloat16 [8192, 2048], P('tp', 'fs'), may hold values from -0.0625 to 0.0625
Outputs:
- layer_out: bfloat16 [8192, 2048], P(('fs', 'tp'))
The draws below stay inside these ranges and needn't reach their ends.
Inputs may be any that keep to these rules, and one draw needn't show every extreme that they name: `decay_rate`: decay rates per position, one for each head.
All inputs are finite; a program needn't handle non-finite values.
Results may differ from the reference program's by a relative error of at most 0.038.
Values may be sent and summed in bfloat16 or wider, within the bound.
A program may use at most 64 MiB of HBM per device.

```python
import jax
import jax.numpy as jnp
from jax import lax

D = 2048
HEADS = 8
DK = 128
DV = 256
FF = 8192
BLOCK = 128
LENGTH = 512
TOKENS = 8192
N_TP = 4


def draw_decay_rate(key, part):
    order_key, quick_key, slow_key = jax.random.split(key, 3)
    ranking = jax.random.permutation(order_key, HEADS)
    quick_rate = jnp.exp(jax.random.uniform(quick_key, (HEADS,), jnp.float32, jnp.log(1.0 / 50.0), jnp.log(1.0 / 30.0)))
    slow_rate = jax.random.uniform(slow_key, (HEADS,), jnp.float32, 0.2, 1.0) * (2.3 / LENGTH)
    return jnp.where(ranking < HEADS // 2, quick_rate, slow_rate)


def levels(rng, shape, cuts, low, largest):
    def one(position, shards_of):
        draws = jax.random.uniform(jax.random.fold_in(jax.random.fold_in(rng, 6), position), (shards_of,), jnp.float32, low / len(cuts), largest / len(cuts))
        return jnp.repeat(jnp.exp(draws), shape[position] // shards_of).reshape((-1,) + (1,) * (len(shape) - position - 1))

    level = one(*cuts[0])
    for cut in cuts[1:]:
        level = level * one(*cut)
    return level


def scatter_about(own_key, shape, scale, limit, pieces=(), held_as=jnp.bfloat16):
    drawn = jax.random.normal(own_key, shape, jnp.float32) * scale
    if len(pieces) > 0:
        drawn = levels(own_key, shape, pieces, -0.22, 0.18) * drawn
    return jnp.clip(drawn, min=-limit, max=limit).astype(held_as)


def setup_inputs(seed: int = 0) -> dict:
    key_list = jax.random.split(jax.random.key(seed), 12)
    resid = scatter_about(key_list[0], (TOKENS, D), 1.0, 6.0, ((0, 32),))
    mix_gain = jnp.clip(1.0 + 0.18 * jax.random.normal(key_list[1], (D,), jnp.float32), 0.1, 1.9)
    w_query = scatter_about(key_list[2], (D, HEADS * DK), D ** -0.5, 0.125, ((0, 8), (1, 4)))
    w_key = scatter_about(key_list[3], (D, HEADS * DK), D ** -0.5, 0.125, ((0, 8), (1, 4)))
    w_value = scatter_about(key_list[4], (D, HEADS * DV), D ** -0.5, 0.125, ((0, 8), (1, 4)))
    w_gate = scatter_about(key_list[5], (D, HEADS * DV), D ** -0.5, 0.125, ((0, 8), (1, 4)))
    w_output = scatter_about(key_list[6], (HEADS * DV, D), (HEADS * DV) ** -0.5, 0.125, ((0, 4), (1, 8)))
    decay_rate = draw_decay_rate(jax.random.fold_in(key_list[11], 71), 0)
    mlp_gain = jnp.clip(1.0 + 0.18 * jax.random.normal(key_list[8], (D,), jnp.float32), 0.1, 1.9)
    w_up = scatter_about(key_list[9], (D, FF), D ** -0.5, 0.125, ((0, 8), (1, 4)))
    w_down = scatter_about(key_list[10], (FF, D), FF ** -0.5, 0.0625, ((0, 4), (1, 8)))
    return dict(resid=resid, mix_gain=mix_gain, w_query=w_query, w_key=w_key, w_value=w_value, w_gate=w_gate, w_output=w_output, decay_rate=decay_rate, mlp_gain=mlp_gain, w_up=w_up, w_down=w_down)


epsilon = 1e-06

def rms_scale(source, gains):
    widened = source.astype(jnp.float32)
    scaled = widened * lax.rsqrt(lax.optimization_barrier(jnp.mean(widened * widened, axis=-1, keepdims=True)) + epsilon)
    return (scaled * gains).astype(jnp.bfloat16)

def retention(queries, key_rows, values, rates):
    seq_count, length, head_count, key_width = queries.shape
    value_width = values.shape[-1]
    block_count = length // BLOCK
    queries = queries.reshape(seq_count, block_count, BLOCK, head_count, key_width)
    key_rows = key_rows.reshape(seq_count, block_count, BLOCK, head_count, key_width) * key_width ** (-0.5)
    values = values.reshape(seq_count, block_count, BLOCK, head_count, value_width)
    places = jnp.arange(BLOCK, dtype=jnp.float32)
    offset = places[:, None] - places[None, :]
    causal = offset >= 0
    inner_decay = jnp.where(causal[None], jnp.exp(-rates[:, None, None] * jnp.where(causal, offset, 0.0)[None]), 0.0)
    scores = jnp.einsum('bnihd,bnjhd->bnhij', queries, key_rows) * inner_decay[None, None]
    within = jnp.einsum('bnhij,bnjhe->bnihe', scores, values)
    key_decayed = key_rows * jnp.exp(-rates[None, :] * (BLOCK - 1.0 - places)[:, None])[None, None, :, :, None]
    updates = jnp.einsum('bnjhd,bnjhe->nbhde', key_decayed, values)
    carry_decay = jnp.exp(-rates * BLOCK)[None, :, None, None]

    def advance(memory, update):
        return (carry_decay * memory + update, memory)
    _, before = lax.scan(advance, jnp.zeros((seq_count, head_count, key_width, value_width), jnp.float32), updates)
    query_decayed = queries * jnp.exp(-rates[None, :] * (places + 1.0)[:, None])[None, None, :, :, None]
    carried = jnp.einsum('bnihd,nbhde->bnihe', query_decayed, before)
    mixed = (within + carried).reshape(seq_count, length, head_count, value_width)
    centre = lax.optimization_barrier(jnp.mean(mixed, axis=-1, keepdims=True))
    spread = lax.optimization_barrier(jnp.mean(jnp.square(mixed - centre), axis=-1, keepdims=True))
    return (mixed - centre) * lax.rsqrt(spread + epsilon)

def heads_view(source, width):
    return source.astype(jnp.float32).reshape(-1, LENGTH, source.shape[1] // width, width)

def grouped_sum(left, right):
    group = left.shape[1] // N_TP
    result = jnp.zeros((left.shape[0], right.shape[1]), jnp.float32)
    for member in range(N_TP):
        partial_sum = jnp.dot(left[:, member * group:(member + 1) * group], right[member * group:(member + 1) * group], preferred_element_type=jnp.float32)
        result = result + lax.optimization_barrier(partial_sum.astype(jnp.bfloat16)).astype(jnp.float32)
    return result

def reference(resid, mix_gain, w_query, w_key, w_value, w_gate, w_output, decay_rate, mlp_gain, w_up, w_down):
    tokens = resid.shape[0]
    normed = rms_scale(resid, mix_gain)

    def project(weight):
        return jnp.dot(normed, weight, preferred_element_type=jnp.float32).astype(jnp.bfloat16)
    queries = project(w_query)
    key_rows = project(w_key)
    values = project(w_value)
    gate_rows = project(w_gate)
    grouped = retention(heads_view(queries, DK), heads_view(key_rows, DK), heads_view(values, DV), decay_rate)
    gated = (jax.nn.silu(gate_rows.astype(jnp.float32)) * grouped.reshape(tokens, -1)).astype(jnp.bfloat16)
    mix_sum = grouped_sum(gated, w_output)
    after_mix = (resid.astype(jnp.float32) + mix_sum).astype(jnp.bfloat16)
    normed_mlp = rms_scale(after_mix, mlp_gain)
    lifted = jnp.dot(normed_mlp, w_up, preferred_element_type=jnp.float32)
    hidden = jnp.square(jax.nn.relu(lifted)).astype(jnp.bfloat16)
    mlp_sum = grouped_sum(hidden, w_down)
    return (after_mix.astype(jnp.float32) + mlp_sum).astype(jnp.bfloat16)
```

```python
import functools

import jax
import jax.numpy as jnp
from jax import lax
from jax.experimental import pallas as pl
from jax.experimental.pallas import tpu as pltpu
from jax.sharding import PartitionSpec as P

DK = 128
DV = 256
LENGTH = 512
MESH = pl.DeviceIdType.MESH
EPS = 1e-06
F32 = jnp.float32
BF16 = jnp.bfloat16


def tile_of(width):
    return 256 if width % 256 == 0 else 128


def kernel(fs, tp, resid_ref, mix_gain_ref, mlp_gain_ref, rate_ref, w1_ref, w2_ref, w3_ref, w4_ref, wo_ref, wu_ref, wd_ref,
           out_ref, wq, wo, wu, wd, xn, xn2, proj, gated, hidden, part1, core1, chip1, part2, chip2,
           after, ring_send, ring_recv, own_sem, in_sem, fold_send, fold_recv, put_send, put_recv,
           tok_send, tok_recv, gate_send, gate_recv, aside_send, aside_recv, over_send, over_recv, line_send, line_recv,
           swap_send, swap_recv, core1_send, core1_recv, chip1_send, chip1_recv, all_send, all_recv,
           core2_send, core2_recv, chip2_send, chip2_recv):
    half = fs // 2
    lines = fs // 2
    in_refs = (w1_ref, w2_ref, w3_ref, w4_ref)
    deep_q = w1_ref.shape[0]
    chips = tp // 2
    rows = resid_ref.shape[0]
    heads = rate_ref.shape[0]
    tokens = rows * tp
    me_f = lax.axis_index("fs")
    me_t = lax.axis_index("tp")
    pair = me_f % 2
    line = me_f // 2
    other_f = 2 * line + 1 - pair
    chip = me_t // 2
    core = me_t % 2
    other_t = 2 * chip + 1 - core

    def place(i):
        col = i % 2
        at = i // 2
        return at * (1 - col) + (fs - 1 - at) * col

    def index(p):
        col = p // half
        return 2 * (p * (1 - col) + (fs - 1 - p) * col) + col

    my_place = place(me_f)
    target = (index((my_place + 1) % fs), index((my_place + fs - 1) % fs))

    def owner(way, dist):
        if way == 0:
            return index((my_place + fs - dist) % fs)
        return index((my_place + dist) % fs)

    def peer(d):
        return (me_t + d) % tp

    def beside(e):
        return 2 * ((chip + e) % chips) + core

    def step_to(way):
        return me_f + 2 if way == 0 else me_f - 2

    def line_has(way, dist):
        return line >= dist if way == 0 else line + dist <= lines - 1

    def line_next(way):
        return line_has(1 - way, 1)

    upper = line // (lines // 2)
    mate_line = (1 - upper) * (1 - line) + upper * (2 * lines - 3 - line)
    mate_f = 2 * mate_line + pair
    all_fold = lines - 2 == 2
    is_end = jnp.logical_or(line == 0, line == lines - 1)
    inner = jnp.logical_not(is_end)
    folds = inner if all_fold else jnp.logical_or(line == 1, line == lines - 2)
    ring_out = (upper + pair == 1, upper + pair != 1)
    line_out = (upper == 1, upper == 0)

    def when(on, run):
        if on is None:
            run()
        else:
            pl.when(on)(run)

    first_row = pl.multiple_of(me_f * deep_q, deep_q)
    loads = []
    for head in range(heads):
        left = 0
        for ref in in_refs:
            w = ref.shape[1] // heads
            copy = pltpu.make_async_copy(
                ref.at[:, head * w:(head + 1) * w],
                wq.at[head, pl.ds(first_row, deep_q), left:left + w], in_sem.at[len(loads)])
            copy.start()
            loads.append(copy)
            left += w

    barrier = pltpu.get_barrier_semaphore()

    def greet(where):
        pl.semaphore_signal(barrier, inc=1, device_id=where, device_id_type=MESH)

    for way in range(2):
        greet((target[way], me_t))
    for d in range(1, tp):
        greet((me_f, peer(d)))
        if d % 2 == 0:
            greet((other_f, peer(d)))
    greet((other_f, me_t))
    for way in range(2):
        at = (line + (1 if way == 0 else lines - 1)) % lines
        greet((2 * at + pair, me_t))
    pl.semaphore_wait(barrier, 2 + (tp - 1) + (chips - 1) + 1 + 2)

    started = []

    def go(copy, on=None):
        if on is None:
            copy.start()
        else:
            @pl.when(on)
            def _():
                copy.start()
        started.append((copy, on))

    def remote(src, dst, s_sem, r_sem, where):
        return pltpu.make_async_remote_copy(
            src_ref=src, dst_ref=dst, send_sem=s_sem, recv_sem=r_sem, device_id=where,
            device_id_type=MESH)

    def landed(dst, s_sem, r_sem):
        return remote(dst, dst, s_sem, r_sem, (me_f, other_t))

    def span(at, size):
        return pl.ds(pl.multiple_of(at, size), size)

    def half_of(way, turn):
        return turn if way == 0 else 1 - turn

    def ring_rounds(half_ring):
        found = []
        for dist in range(1, half_ring):
            found += [(dist, 0), (dist, 1)]
        return found + [(half_ring, 0)]

    rounds = ring_rounds(half)
    per = len(rounds)
    out_rows = wo_ref.shape[0] // 2

    def slot(who, h):
        return wo.at[who, pl.ds(h * out_rows, out_rows), :]

    ring = []
    for n, (dist, turn) in enumerate(rounds):
        pair_of = []
        for way in range(2):
            h = half_of(way, turn)
            who = owner(way, dist - 1)
            src = wo_ref.at[pl.ds(h * out_rows, out_rows), :] if dist == 1 else slot(who, h)
            pair_of.append((
                remote(src, slot(who, h), ring_send.at[way, n], ring_recv.at[way, n], (target[way], me_t)),
                landed(slot(owner(way, dist), h), ring_send.at[way, n], ring_recv.at[way, n])))
            started.append((pair_of[-1][0], None))
        ring.append(pair_of)

    def send(n, ways=(0, 1), out=None):
        for way in ways:
            copy = ring[n][way][0]
            if out is None:
                copy.start()
            else:
                pl.when(ring_out[way] if out else jnp.logical_not(ring_out[way]))(copy.start)

    def arrive(n, out):
        dist, turn = rounds[n]
        more = dist + 1 < half or (dist + 1 == half and turn == 0)
        for way in range(2):
            def run():
                ring[n][way][1].wait_recv()
                if more:
                    send(n + 2, (way,))
            pl.when(ring_out[way] if out else jnp.logical_not(ring_out[way]))(run)

    count_in = 2 * (lines - 2)
    half_in = count_in // 2

    def place_in(i):
        col = i % 2
        at = i // 2 - 1
        return at * (1 - col) + (count_in - 1 - at) * col

    def index_in(p):
        col = p // half_in
        return 2 * (p * (1 - col) + (count_in - 1 - p) * col + 1) + col

    my_in = (place_in(me_f) + count_in) % count_in
    target_in = (index_in((my_in + 1) % count_in), index_in((my_in + count_in - 1) % count_in))

    def owner_in(way, dist):
        return index_in((my_in + (count_in - dist if way == 0 else dist)) % count_in)

    def mate_of(who):
        at = who // 2
        up = at // (lines // 2)
        return 2 * ((1 - up) * (1 - at) + up * (2 * lines - 3 - at)) + who % 2

    def fold_of(who):
        return jnp.logical_or(who // 2 == 1, who // 2 == lines - 2)

    part_q = deep_q // 2

    def slot_in(head, who, h):
        return wq.at[head, pl.ds(pl.multiple_of(who * deep_q + h * part_q, part_q), part_q), :]

    rounds_in = ring_rounds(half_in)
    per_in = len(rounds_in)
    ring_in = []
    for head in range(heads):
        for s in range(2):
            for dist, turn in rounds_in:
                n = len(ring_in)
                pair_of = []
                for way in range(2):
                    h = half_of(way, turn)
                    gone, come = owner_in(way, dist - 1), owner_in(way, dist)
                    on_out = None if s == 0 or all_fold else fold_of(gone)
                    on_in = None if s == 0 or all_fold else fold_of(come)
                    if s == 1:
                        gone, come = mate_of(gone), mate_of(come)
                    out = remote(slot_in(head, gone, h), slot_in(head, gone, h), fold_send.at[way, n],
                                 fold_recv.at[way, n], (target_in[way], me_t))
                    back = landed(slot_in(head, come, h), fold_send.at[way, n], fold_recv.at[way, n])
                    pair_of.append((out, on_out, back, on_in))
                    started.append((out, inner if on_out is None else jnp.logical_and(inner, on_out)))
                ring_in.append(pair_of)

    def send_in(n):
        for out, on_out, _, _ in ring_in[n]:
            when(on_out, out.start)

    def arrive_in(n):
        for _, _, back, on_in in ring_in[n]:
            when(on_in, back.wait_recv)
        dist, turn = rounds_in[n % per_in]
        if dist + 1 < half_in or (dist + 1 == half_in and turn == 0):
            send_in(n + 2)

    def rows_in(head, who):
        return wq.at[head, pl.ds(pl.multiple_of(who * deep_q, deep_q), deep_q), :]

    puts, puts_in = [], []
    for head in range(heads):
        puts.append(remote(rows_in(head, me_f), rows_in(head, me_f), put_send.at[head], put_recv.at[head],
                           (mate_f, me_t)))
        puts_in.append(landed(rows_in(head, mate_f), put_send.at[head], put_recv.at[head]))
        started.append((puts[-1], is_end))

    up_cols = wu.shape[1]
    deep = wu_ref.shape[0]
    down_rows = wd.shape[1]

    def piece(g, who):
        return wu.at[span(who * deep, deep), :] if g == 0 else wd.at[who]

    def share(g, y):
        if g == 0:
            return wu_ref.at[:, span(y * up_cols, up_cols)]
        return wd_ref.at[span(y * down_rows, down_rows), :]

    line_rounds = [(g, dist, turn) for g in range(2) for dist in range(1, lines) for turn in range(2)]
    per_line = 2 * (lines - 1)

    def line_owner(way, dist, turn):
        at = line - dist if way == 0 else line + dist
        return 2 * at + (pair if turn == 0 else 1 - pair)

    to_end = (line == lines - 2, line == 1)
    line_copies = []
    for m, (g, dist, turn) in enumerate(line_rounds):
        both = []
        for way in range(2):
            who = line_owner(way, dist - 1, turn)
            src = share(g, pair) if dist == 1 and turn == 0 else piece(g, who)
            on = line_next(way) if dist == 1 else jnp.logical_and(line_next(way), line_has(way, dist - 1))
            has = line_has(way, dist)
            if dist == 1 and turn == 1:
                on = jnp.logical_and(on, jnp.logical_not(to_end[way]))
                has = jnp.logical_and(has, inner)
            copy = remote(src, piece(g, who), line_send.at[way, m], line_recv.at[way, m],
                          (step_to(way), me_t))
            back = landed(piece(g, line_owner(way, dist, turn)), line_send.at[way, m],
                          line_recv.at[way, m])
            both.append((copy, on, back, has))
            started.append((copy, on))
        line_copies.append(both)

    def line_send_round(m, ways=(0, 1), out=None):
        for way in ways:
            copy, on, _, _ = line_copies[m][way]
            if out is not None:
                on = jnp.logical_and(on, line_out[way] if out else jnp.logical_not(line_out[way]))
            pl.when(on)(copy.start)

    def line_arrive(m, out):
        g, dist, turn = line_rounds[m]
        for way in range(2):
            def run():
                _, _, back, has = line_copies[m][way]
                pl.when(has)(back.wait_recv)
                if dist + 1 < lines:
                    line_send_round(m + 2, (way,))
            pl.when(line_out[way] if out else jnp.logical_not(line_out[way]))(run)

    aside, aside_in, across_end, across_in = [], [], [], []
    for g in range(2):
        if g == 0:
            stash = xn.at[tokens:tokens + deep, :up_cols]
        else:
            stash = xn.at[tokens:tokens + down_rows, up_cols:up_cols + wd.shape[2]]
        aside.append(remote(share(g, 1 - pair), stash, aside_send.at[g], aside_recv.at[g], (mate_f, me_t)))
        aside_in.append(landed(stash, aside_send.at[g], aside_recv.at[g]))
        across_end.append(remote(stash, piece(g, mate_f), over_send.at[g], over_recv.at[g], (other_f, me_t)))
        across_in.append(landed(piece(g, 2 * mate_line + 1 - pair), over_send.at[g], over_recv.at[g]))
        started.append((aside[-1], folds))
        started.append((across_end[-1], is_end))

    swaps, swaps_in = [], []
    for g in range(2):
        swaps.append(remote(share(g, 1 - pair), piece(g, me_f), swap_send.at[g], swap_recv.at[g],
                            (other_f, me_t)))
        swaps_in.append(landed(piece(g, other_f), swap_send.at[g], swap_recv.at[g]))
        started.append((swaps[-1], None))

    own = [None]
    for n, (src, dst) in enumerate((
            (wo_ref, wo.at[me_f]),
            (share(0, pair), piece(0, me_f)),
            (share(1, pair), piece(1, me_f)))):
        copy = pltpu.make_async_copy(src, dst, own_sem.at[n])
        own.append(copy)

    my_rows = span(me_t * rows, rows)

    def norm(source, gain_ref):
        wide = source.astype(F32)
        mean = jnp.mean(wide * wide, axis=-1, keepdims=True)
        return (wide * lax.rsqrt(mean + EPS) * gain_ref[...]).astype(BF16)

    step = 64

    def norm_into(buf, first, source_ref, gain_ref):
        @pl.loop(0, rows // step)
        def _(i):
            at = pl.multiple_of(i * step, step)
            buf[pl.ds(pl.multiple_of(first + at, step), step), :] = norm(
                source_ref[pl.ds(at, step), :], gain_ref)

    half_rows = rows // 2

    def tok(group, t, part=None):
        first = group * tokens + t * rows
        if part is None:
            return xn.at[span(first, rows), :]
        return xn.at[pl.ds(pl.multiple_of(first + part * half_rows, half_rows), half_rows), :]

    xn_sends = []
    tok_count = [0]

    def tok_pair(out_ref, in_ref, where, on):
        n = tok_count[0]
        tok_count[0] += 1
        out = remote(out_ref, out_ref, tok_send.at[n], tok_recv.at[n], where)
        xn_sends.append((out, on))
        return out, landed(in_ref, tok_send.at[n], tok_recv.at[n])

    def tok_set(group, part, on):
        core_c = tok_pair(tok(group, me_t, part), tok(group, other_t, part), (me_f, other_t), on)
        over, pass_on = [], []
        for e in range(1, chips):
            t = beside(chips - e)
            over.append(tok_pair(tok(group, me_t, part), tok(group, t, part), (me_f, beside(e)), on))
            pass_on.append(tok_pair(
                tok(group, t, part),
                tok(group, 2 * ((chip + chips - e) % chips) + 1 - core, part), (me_f, other_t), on))
        return core_c, over, pass_on

    own_set = tok_set(1, None, inner)
    mate_sets = [tok_set(0, part, folds) for part in range(2)]
    to_mate = [tok_pair(tok(0, me_t, part), tok(0, me_t, part), (mate_f, me_t), is_end) for part in range(2)]

    def tok_start(which):
        which[0][0].start()
        for out, _ in which[1]:
            out.start()

    def tok_pass(which):
        for (_, back), (out, _) in zip(which[1], which[2]):
            back.wait_recv()
            out.start()

    def tok_wait(which):
        which[0][1].wait_recv()
        for _, back in which[2]:
            back.wait_recv()

    def mate_tokens(part):
        def run():
            to_mate[part][1].wait_recv()
            tok_start(mate_sets[part])
        return lambda: when(None if all_fold else folds, run)

    def mate_pass(part):
        return lambda: when(None if all_fold else folds, lambda: tok_pass(mate_sets[part]))

    gates, gates_in = [], []
    for head in range(heads):
        cut = slice(head * DV, (head + 1) * DV)
        gates.append(remote(gated.at[0, :, cut], gated.at[1, :, cut], gate_send.at[head], gate_recv.at[head],
                            (mate_f, me_t)))
        gates_in.append(landed(gated.at[1, :, cut], gate_send.at[head], gate_recv.at[head]))
        started.append((gates[-1], folds))

    def project(group, head):
        width = proj.shape[1]
        t = tile_of(width)

        @pl.loop(0, width // t)
        def _(j):
            cols = pl.ds(pl.multiple_of(j * t, t), t)
            proj[:, cols] = jnp.dot(xn[group * tokens:(group + 1) * tokens, :], wq[head, :, cols],
                                    preferred_element_type=F32).astype(BF16)

    def retain(group, head):
        rate = rate_ref[head]

        @pl.loop(0, tokens // LENGTH)
        def _(n):
            base = pl.multiple_of(n * LENGTH, LENGTH)
            rs = pl.ds(base, LENGTH)
            q = proj[rs, :DK]
            k = proj[rs, DK:2 * DK]
            v = proj[rs, 2 * DK:2 * DK + DV]
            g = proj[rs, 2 * DK + DV:].astype(F32)
            scores = lax.dot_general(q, k, (((1,), (1,)), ((), ())), preferred_element_type=F32)
            t_at = lax.broadcasted_iota(jnp.int32, (LENGTH, LENGTH), 0)
            s_at = lax.broadcasted_iota(jnp.int32, (LENGTH, LENGTH), 1)
            gap = t_at - s_at
            decay = jnp.exp(-rate * jnp.maximum(gap, 0).astype(F32)) * (DK ** -0.5)
            scores = jnp.where(gap >= 0, scores * decay, 0.0).astype(BF16)
            mixed = jnp.dot(scores, v, preferred_element_type=F32)
            mean = jnp.mean(mixed, axis=-1, keepdims=True)
            off = mixed - mean
            var = jnp.mean(off * off, axis=-1, keepdims=True)
            grouped = off * lax.rsqrt(var + EPS)
            gated[group, rs, head * DV:(head + 1) * DV] = (g / (1.0 + jnp.exp(-g)) * grouped).astype(BF16)

    def heads_of(group, head):
        project(group, head)
        retain(group, head)
        if group == 0:
            gates[head].start()

    def mate_heads(head):
        when(None if all_fold else folds, lambda: heads_of(0, head))

    def mix_block(x, c):
        return part1.at[span((2 * x + c) * rows, rows), :]

    def mix_out():
        cols = wo.shape[2]

        @pl.loop(0, fs)
        def _(j):
            part1[:, span(j * cols, cols)] = jnp.dot(
                gated[1], wo[j], preferred_element_type=F32).astype(BF16)
        order = [e % chips for e in range(1, chips + 1)]
        for e in order:
            x = (chip + e) % chips
            go(remote(mix_block(x, 1 - core), core1.at[e], core1_send.at[e], core1_recv.at[e],
                      (me_f, other_t)))
        for e in order:
            landed(core1.at[e], core1_send.at[e], core1_recv.at[e]).wait_recv()
            if e:
                first = beside(e) * rows

                @pl.loop(0, rows // step)
                def _(i):
                    at = pl.ds(pl.multiple_of(first + i * step, step), step)
                    more = core1[e, span(i * step, step), :].astype(F32)
                    part1[at, :] = (part1[at, :].astype(F32) + more).astype(BF16)
                go(remote(ag_mix(beside(e)), chip1.at[e - 1], chip1_send.at[e - 1],
                          chip1_recv.at[e - 1], (me_f, beside(e))))

    def ag_mix(t):
        return part1.at[span(t * rows, rows), :]

    def mix_end():
        for e in range(1, chips):
            landed(chip1.at[e - 1], chip1_send.at[e - 1], chip1_recv.at[e - 1]).wait_recv()

        @pl.loop(0, rows // step)
        def _(i):
            at = span(i * step, step)
            total = part1[pl.ds(pl.multiple_of(me_t * rows + i * step, step), step), :].astype(F32)
            total = total + core1[0, at, :].astype(F32)
            for e in range(1, chips):
                total = total + chip1[e - 1, at, :].astype(F32)
            sum_ = (resid_ref[at, :].astype(F32) + total).astype(BF16)
            after[at, :] = sum_
            xn2[pl.ds(pl.multiple_of(block(pair, me_t) * rows + i * step, step), step), :] = norm(
                sum_, mlp_gain_ref)

    def block(y, t):
        return (t % 2) * (2 * chips) + y * chips + t // 2

    def wide(y, t, part=None):
        first = block(y, t) * rows
        hr = rows // 2
        if part is None:
            return xn2.at[span(first, rows), :]
        return xn2.at[pl.ds(pl.multiple_of(first + part * hr, hr), hr), :]

    more_chips = chips - 1
    pieces = 1 + 3 * more_chips

    def all_copy(n, ref, where):
        go(remote(ref, ref, all_send.at[n], all_recv.at[n], where))

    def all_landed(n, ref):
        landed(ref, all_send.at[n], all_recv.at[n]).wait_recv()

    def across(n, ref):
        all_copy(pieces + n, ref, (me_f, other_t))

    def all_first():
        ref = wide(pair, me_t)
        all_copy(0, ref, (other_f, me_t))
        for e in range(1, chips):
            all_copy(e, ref, (me_f, beside(e)))
        all_copy(2 * pieces, ref, (me_f, other_t))

    def all_second():
        ref = wide(1 - pair, me_t)
        all_landed(0, ref)
        for e in range(1, chips):
            all_copy(more_chips + e, wide(1 - pair, me_t, 0), (me_f, beside(e)))
        across(0, ref)
        for e in range(1, chips):
            t = beside(chips - e)
            all_landed(e, wide(pair, t))
            all_copy(2 * more_chips + e, wide(pair, t, 1), (other_f, me_t))
            across(e, wide(pair, t))

    def all_beside():
        all_landed(2 * pieces, wide(pair, other_t))
        for e in range(1, chips):
            t = 2 * ((chip + chips - e) % chips) + 1 - core
            all_landed(pieces + e, wide(pair, t))

    def all_third():
        for part in range(2):
            for e in range(1, chips):
                n = (1 + part) * more_chips + e
                ref = wide(1 - pair, beside(chips - e), part)
                all_landed(n, ref)
                across(n, ref)
        all_landed(pieces, wide(1 - pair, other_t))
        for e in range(1, chips):
            t = 2 * ((chip + chips - e) % chips) + 1 - core
            for part in range(2):
                all_landed(pieces + (1 + part) * more_chips + e, wide(1 - pair, t, part))

    def lift(y):
        t = tile_of(up_cols)
        size = chips * rows

        @pl.loop(0, up_cols // t)
        def _(j):
            cols = span(j * t, t)

            @pl.loop(0, 2)
            def _(i):
                at = span(i * tokens + y * size, size)
                up = jnp.maximum(jnp.dot(xn2[at, :], wu[:, cols], preferred_element_type=F32), 0.0)
                hidden[at, cols] = (up * up).astype(BF16)

    cw = wd.shape[2]
    r2 = 2 * chips - 1

    def lower_copy(who, n, ref, where):
        dst = chip2.at[n, :, span(who * cw, cw)]
        out = remote(ref, dst, chip2_send.at[n, who], chip2_recv.at[n, who], where)
        return out, landed(dst, chip2_send.at[n, who], chip2_recv.at[n, who])

    def part_rows(y, t):
        return span(block(y, t) * rows, rows)

    def along_chips(who, cols):
        first, second = [], []
        for e in range(1, chips):
            for y in range(2):
                first.append(lower_copy(who, 2 * (e - 1) + y, part2.at[part_rows(y, beside(e)), cols],
                                        (me_f, beside(e))))
        second.append(lower_copy(who, r2 - 1, part2.at[part_rows(1 - pair, me_t), cols], (other_f, me_t)))

        def add():
            at = part_rows(1 - pair, me_t)
            total = part2[at, cols].astype(F32)
            for e in range(1, chips):
                total = total + chip2[2 * (e - 1) + 1 - pair, :, cols].astype(F32)
            part2[at, cols] = total.astype(BF16)

        def rest():
            total = chip2[r2 - 1, :, cols].astype(F32)
            for e in range(1, chips):
                total = total + chip2[2 * (e - 1) + pair, :, cols].astype(F32)
            return total
        return first, second, add, rest

    def across_pair(who, cols):
        first, second = [], []
        for e in range(chips):
            first.append(lower_copy(who, e, part2.at[part_rows(1 - pair, beside(e)), cols], (other_f, me_t)))
        for e in range(1, chips):
            second.append(lower_copy(who, chips + e - 1, part2.at[part_rows(pair, beside(e)), cols],
                                     (me_f, beside(e))))

        def add():
            for e in range(1, chips):
                at = part_rows(pair, beside(e))
                part2[at, cols] = (part2[at, cols].astype(F32) + chip2[e, :, cols].astype(F32)).astype(BF16)

        def rest():
            total = chip2[0, :, cols].astype(F32)
            for e in range(1, chips):
                total = total + chip2[chips + e - 1, :, cols].astype(F32)
            return total
        return first, second, add, rest

    finals, middles = [], []

    def lower(who, on=None):
        cols = span(who * cw, cw)
        mine = part_rows(pair, me_t)
        side = remote(part2.at[span((1 - core) * tokens, tokens), cols], xn.at[pl.ds(0, tokens), cols],
                      core2_send.at[who], core2_recv.at[who], (me_f, other_t))
        side_in = landed(xn.at[pl.ds(0, tokens), cols], core2_send.at[who], core2_recv.at[who])
        plans = [(who % 2 == 0, along_chips(who, cols)), (who % 2 == 1, across_pair(who, cols))]

        def run():
            @pl.loop(0, 2)
            def _(i):
                at = span(((1 - core) * (1 - i) + core * i) * tokens, tokens)
                part2[at, cols] = jnp.dot(
                    hidden[at, :], wd[who], preferred_element_type=F32).astype(BF16)

                @pl.when(i == 0)
                def _():
                    side.start()
            side_in.wait_recv()

            @pl.loop(0, tokens // 128)
            def _(i):
                at = pl.ds(pl.multiple_of(core * tokens + i * 128, 128), 128)
                more = xn[span(i * 128, 128), cols].astype(F32)
                part2[at, cols] = (part2[at, cols].astype(F32) + more).astype(BF16)
            for this, (first, _, _, _) in plans:
                def begin():
                    for out, _ in first:
                        out.start()
                pl.when(this)(begin)

        def middle():
            for this, (first, second, add, _) in plans:
                def pass_on():
                    for _, back in first:
                        back.wait_recv()
                    add()
                    for out, _ in second:
                        out.start()
                pl.when(this)(pass_on)

        def end():
            for this, (first, second, _, rest) in plans:
                def close():
                    for _, back in second:
                        back.wait_recv()
                    total = part2[mine, cols].astype(F32) + rest()
                    out_ref[:, cols] = (after[:, cols].astype(F32) + total).astype(BF16)
                    for out, _ in first + second:
                        out.wait_send()
                pl.when(this)(close)
            side.wait_send()

        when(on, run)
        middles.append((middle, on))
        finals.append((end, on))
        if len(middles) > 2:
            then, at = middles[-3]
            when(at, then)

    if all_fold:
        inner_order = [[(0, False), (1, False), (0, True), (1, True)],
                       [(2, False), (3, False), (2, True), (3, True)], [(4, False), (5, False)],
                       [(4, True), (5, True)], [(6, True), (6, False)]]
        end_order = [[(0, False), (1, False), (0, True), (1, True), (2, False), (3, False)],
                     [(2, True), (3, True), (4, False)], [(5, False), (4, True), (5, True), (6, True), (6, False)]]
    else:
        by_round = [(n, out) for n in range(per) for out in (False, True)]
        inner_order = [[], [], [], [], by_round]
        end_order = [[], [], by_round]

    def arrivals(part):
        for n, out in part:
            arrive(n, out)

    def inner_front():
        send(0, out=True)
        send(1, out=True)
        line_send_round(0, out=True)

        when(None if all_fold else folds, aside[0].start)
        line_send_round(per_line, out=True)
        when(None if all_fold else folds, aside[1].start)
        for copy in loads:
            copy.wait()
        send_in(0)
        send_in(1)
        norm_into(xn, tokens + me_t * rows, resid_ref, mix_gain_ref)
        tok_start(own_set)
        for copy in own[1:]:
            copy.start()
        hooks = {(0, 1, 0): mate_tokens(0), (0, 1, 1): lambda: tok_pass(own_set),
                 (1, 0, 0): mate_tokens(1), (1, 0, 2): mate_pass(0), (1, 1, 0): mate_pass(1)}
        order = list(hooks)

        def drain(upto):
            while order and order[0] <= upto:
                hooks[order.pop(0)]()

        for head in range(heads):
            last = head == heads - 1
            first = 2 * head * per_in
            for n in range(per_in):
                arrive_in(first + n)
                drain((head, 0, n))
                if n == 1:
                    if last:
                        send(0, out=False)
                        send(1, out=False)

                    def pushed():
                        puts_in[head].wait_recv()
                    when(None if all_fold else folds, pushed)
                    send_in(first + per_in)
                    send_in(first + per_in + 1)
            for n in range(per_in):
                arrive_in(first + per_in + n)
                if n == 0:
                    if last:
                        for g in range(2):
                            swaps[g].start()
                        arrivals(inner_order[0])
                    else:
                        send_in(first + 2 * per_in)
                        send_in(first + 2 * per_in + 1)
                drain((head, 1, n))
                if n == 0 and last:
                    drain((2, 0, 0))
                    for part in range(2):
                        when(None if all_fold else folds, lambda: tok_wait(mate_sets[part]))
                    for early in range(head):
                        mate_heads(early)
                    arrivals(inner_order[1])
            if not last:
                if head == 0:
                    tok_wait(own_set)
                heads_of(1, head)
        if heads == 1:
            tok_wait(own_set)
        arrivals(inner_order[2])
        line_send_round(0, out=False)
        mate_heads(heads - 1)
        arrivals(inner_order[3])
        swaps_in[0].wait_recv()
        line_send_round(1)
        heads_of(1, heads - 1)
        arrivals(inner_order[4])

    def end_front():
        send(0, out=True)
        send(1, out=True)
        for g in range(2):
            swaps[g].start()
        for copy in loads:
            copy.wait()
        puts[0].start()
        norm_into(xn, me_t * rows, resid_ref, mix_gain_ref)
        for out, _ in to_mate:
            out.start()
        for head in range(1, heads):
            puts[head].start()
        send(0, out=False)
        send(1, out=False)
        for copy in own[1:]:
            copy.start()
        arrivals(end_order[0])
        swaps_in[0].wait_recv()
        aside_in[0].wait_recv()
        across_end[0].start()
        line_send_round(0)
        arrivals(end_order[1])
        line_send_round(1)
        aside_in[1].wait_recv()
        across_end[1].start()
        line_send_round(per_line)
        swaps_in[1].wait_recv()
        line_send_round(per_line + 1)
        arrivals(end_order[2])
        for back in gates_in:
            back.wait_recv()

    pl.when(inner)(inner_front)
    pl.when(is_end)(end_front)
    own[1].wait()
    mix_out()
    line_arrive(0, False)
    line_arrive(1, False)

    def inner_down():
        line_send_round(per_line, out=False)
        swaps_in[1].wait_recv()
        line_send_round(per_line + 1)
    pl.when(inner)(inner_down)

    line_arrive(0, True)
    line_arrive(1, True)
    for copy, on in xn_sends:
        pl.when(on)(copy.wait_send)
    mix_end()
    all_first()
    line_arrive(2, False)
    line_arrive(3, False)
    line_arrive(2, True)
    line_arrive(3, True)
    all_second()
    for k in range(4, per_line):
        line_arrive(k, False)
        line_arrive(k, True)
    for k in range(2):
        line_arrive(per_line + k, False)

    def end_landed():
        for back in across_in:
            back.wait_recv()
    pl.when(is_end)(end_landed)
    line_arrive(per_line, True)
    own[2].wait()
    own[3].wait()
    all_beside()
    lift(pair)
    all_third()
    line_arrive(per_line + 1, True)
    lift(1 - pair)
    lower(me_f)
    lower(other_f)
    for m in range(per_line, 2 * per_line):
        if m + 2 < 2 * per_line:
            line_arrive(m + 2, False)
        _, dist, turn = line_rounds[m]
        if m >= per_line + 2:
            line_arrive(m, True)
        for way in range(2):
            lower(line_owner(way, dist, turn), line_has(way, dist))

    for then, on in middles[-2:]:
        when(on, then)
    for end, on in finals:
        when(on, end)
    for copy, on in started:
        when(on, copy.wait_send)


def on_device(fs, tp, resid, mix_gain, w_query, w_key, w_value, w_gate, w_output, decay_rate,
              mlp_gain, w_up, w_down):
    rows, width = resid.shape
    tokens = rows * tp
    in_width = w_query.shape[1] + w_key.shape[1] + w_value.shape[1] + w_gate.shape[1]
    chips = tp // 2
    heads = decay_rate.shape[0]
    wide = 2 * (1 + 3 * (chips - 1)) + 1
    vmem = pl.BlockSpec(memory_space=pltpu.VMEM)
    hbm = pl.BlockSpec(memory_space=pl.ANY)
    dma = pltpu.SemaphoreType.DMA
    cols = width // fs
    return pl.pallas_call(
        functools.partial(kernel, fs, tp),
        out_shape=jax.ShapeDtypeStruct((rows, width), BF16),
        in_specs=[vmem] * 3 + [pl.BlockSpec(memory_space=pltpu.SMEM)] + [hbm] * 7,
        out_specs=vmem,
        scratch_shapes=[
            pltpu.VMEM((heads, width, in_width // heads), BF16),
            pltpu.VMEM((fs, w_output.shape[0], cols), BF16),
            pltpu.VMEM((width, w_up.shape[1] // 2), BF16),
            pltpu.VMEM((fs, w_down.shape[0] // 2, cols), BF16),
            pltpu.VMEM((2 * tokens, width), BF16),
            pltpu.VMEM((2 * tokens, width), BF16),
            pltpu.VMEM((tokens, in_width // heads), BF16),
            pltpu.VMEM((2, tokens, w_output.shape[0]), BF16),
            pltpu.VMEM((2 * tokens, w_up.shape[1] // 2), BF16),
            pltpu.VMEM((tokens, width), BF16),
            pltpu.VMEM((chips, rows, width), BF16),
            pltpu.VMEM((chips - 1, rows, width), BF16),
            pltpu.VMEM((2 * tokens, width), BF16),
            pltpu.VMEM((2 * chips - 1, rows, width), BF16),
            pltpu.VMEM((rows, width), BF16),
            dma((2, fs - 1)),
            dma((2, fs - 1)),
            dma((3,)),
            dma((4 * heads,)),
            dma((2, 2 * heads * (fs - 5))),
            dma((2, 2 * heads * (fs - 5))),
            dma((heads,)),
            dma((heads,)),
            dma((3 * (2 * chips - 1) + 2,)),
            dma((3 * (2 * chips - 1) + 2,)),
            dma((heads,)),
            dma((heads,)),
            dma((2,)),
            dma((2,)),
            dma((2,)),
            dma((2,)),
            dma((2, 2 * (fs - 2))),
            dma((2, 2 * (fs - 2))),
            dma((2,)),
            dma((2,)),
            dma((chips,)),
            dma((chips,)),
            dma((chips - 1,)),
            dma((chips - 1,)),
            dma((wide,)),
            dma((wide,)),
            dma((fs,)),
            dma((fs,)),
            dma((2 * chips - 1, fs)),
            dma((2 * chips - 1, fs)),
        ],
        compiler_params=pltpu.CompilerParams(
            collective_id=0, has_side_effects=True, vmem_limit_bytes=67043328),
    )(resid, mix_gain[None, :], mlp_gain[None, :], decay_rate, w_query, w_key, w_value,
      w_gate, w_output, w_up, w_down)


def solution(mesh):
    placed = (
        P(("fs", "tp"), None),
        P(),
        P("fs", "tp"),
        P("fs", "tp"),
        P("fs", "tp"),
        P("fs", "tp"),
        P("tp", "fs"),
        P("tp"),
        P(),
        P("fs", "tp"),
        P("tp", "fs"),
    )
    sizes = dict(mesh.shape)
    return jax.shard_map(
        functools.partial(on_device, sizes["fs"], sizes["tp"]), mesh=mesh, in_specs=placed,
        out_specs=P(("fs", "tp"), None), check_vma=False)
```

```python
import functools

import jax
import jax.numpy as jnp
from jax import lax
from jax.experimental import pallas as pl
from jax.experimental.pallas import tpu as pltpu
from jax.sharding import PartitionSpec as P

DK = 128
DV = 256
LENGTH = 512
MESH = pl.DeviceIdType.MESH
EPS = 1e-06
CHUNKS = 8
F32 = jnp.float32
BF16 = jnp.bfloat16


def tile_of(width):
    return 256 if width % 256 == 0 else 128


def kernel(fs, tp, resid_ref, mix_gain_ref, mlp_gain_ref, rate_ref, w1_ref, w2_ref, w3_ref, w4_ref, wo_ref, wu_ref, wd_ref,
           out_ref, wq, wo, wu, wd, xn, xn2, proj, gated, hidden, part1, core1, chip1, part2, chip2,
           after, ring_send, ring_recv, own_sem, in_sem, fold_send, fold_recv, put_send, put_recv,
           tok_send, tok_recv, gate_send, gate_recv, aside_send, aside_recv, over_send, over_recv, line_send, line_recv,
           swap_send, swap_recv, core1_send, core1_recv, chip1_send, chip1_recv, all_send, all_recv,
           core2_send, core2_recv, chip2_send, chip2_recv):
    half = fs // 2
    lines = fs // 2
    chunks = CHUNKS
    in_refs = (w1_ref, w2_ref, w3_ref, w4_ref)
    deep_q = w1_ref.shape[0]
    chips = tp // 2
    rows = resid_ref.shape[0]
    heads = rate_ref.shape[0]
    tokens = rows * tp
    me_f = lax.axis_index("fs")
    me_t = lax.axis_index("tp")
    pair = me_f % 2
    line = me_f // 2
    other_f = 2 * line + 1 - pair
    chip = me_t // 2
    core = me_t % 2
    other_t = 2 * chip + 1 - core

    def place(i):
        col = i % 2
        at = i // 2
        return at * (1 - col) + (fs - 1 - at) * col

    def index(p):
        col = p // half
        return 2 * (p * (1 - col) + (fs - 1 - p) * col) + col

    my_place = place(me_f)
    target = (index((my_place + 1) % fs), index((my_place + fs - 1) % fs))

    def owner(way, dist):
        if way == 0:
            return index((my_place + fs - dist) % fs)
        return index((my_place + dist) % fs)

    def peer(d):
        return (me_t + d) % tp

    def beside(e):
        return 2 * ((chip + e) % chips) + core

    def step_to(way):
        return me_f + 2 if way == 0 else me_f - 2

    def line_has(way, dist):
        return line >= dist if way == 0 else line + dist <= lines - 1

    def line_next(way):
        return line_has(1 - way, 1)

    upper = line // (lines // 2)
    mate_line = (1 - upper) * (1 - line) + upper * (2 * lines - 3 - line)
    mate_f = 2 * mate_line + pair
    all_fold = lines - 2 == 2
    is_end = jnp.logical_or(line == 0, line == lines - 1)
    inner = jnp.logical_not(is_end)
    folds = inner if all_fold else jnp.logical_or(line == 1, line == lines - 2)
    ring_out = (upper + pair == 1, upper + pair != 1)
    line_out = (upper == 1, upper == 0)

    def when(on, run):
        if on is None:
            run()
        else:
            pl.when(on)(run)

    first_row = pl.multiple_of(me_f * deep_q, deep_q)
    loads = []
    for head in range(heads):
        left = 0
        for ref in in_refs:
            w = ref.shape[1] // heads
            copy = pltpu.make_async_copy(
                ref.at[:, head * w:(head + 1) * w],
                wq.at[head, pl.ds(first_row, deep_q), left:left + w], in_sem.at[len(loads)])
            copy.start()
            loads.append(copy)
            left += w

    barrier = pltpu.get_barrier_semaphore()

    def greet(where):
        pl.semaphore_signal(barrier, inc=1, device_id=where, device_id_type=MESH)

    for way in range(2):
        greet((target[way], me_t))
    for d in range(1, tp):
        greet((me_f, peer(d)))
        if d % 2 == 0:
            greet((other_f, peer(d)))
    greet((other_f, me_t))
    for way in range(2):
        at = (line + (1 if way == 0 else lines - 1)) % lines
        greet((2 * at + pair, me_t))
    pl.semaphore_wait(barrier, 2 + (tp - 1) + (chips - 1) + 1 + 2)

    started = []

    def go(copy, on=None):
        if on is None:
            copy.start()
        else:
            @pl.when(on)
            def _():
                copy.start()
        started.append((copy, on))

    def remote(src, dst, s_sem, r_sem, where):
        return pltpu.make_async_remote_copy(
            src_ref=src, dst_ref=dst, send_sem=s_sem, recv_sem=r_sem, device_id=where,
            device_id_type=MESH)

    def landed(dst, s_sem, r_sem):
        return remote(dst, dst, s_sem, r_sem, (me_f, other_t))

    def span(at, size):
        return pl.ds(pl.multiple_of(at, size), size)

    def half_of(way, turn):
        return turn if way == 0 else 1 - turn

    def ring_rounds(half_ring):
        found = []
        for dist in range(1, half_ring):
            found += [(dist, 0), (dist, 1)]
        return found + [(half_ring, 0)]

    rounds = ring_rounds(half)
    per = len(rounds)
    out_rows = wo_ref.shape[0] // 2

    def slot(who, h):
        return wo.at[who, pl.ds(h * out_rows, out_rows), :]

    ring = []
    for n, (dist, turn) in enumerate(rounds):
        pair_of = []
        for way in range(2):
            h = half_of(way, turn)
            who = owner(way, dist - 1)
            src = wo_ref.at[pl.ds(h * out_rows, out_rows), :] if dist == 1 else slot(who, h)
            pair_of.append((
                remote(src, slot(who, h), ring_send.at[way, n], ring_recv.at[way, n], (target[way], me_t)),
                landed(slot(owner(way, dist), h), ring_send.at[way, n], ring_recv.at[way, n])))
            started.append((pair_of[-1][0], None))
        ring.append(pair_of)

    def send(n, ways=(0, 1), out=None):
        for way in ways:
            copy = ring[n][way][0]
            if out is None:
                copy.start()
            else:
                pl.when(ring_out[way] if out else jnp.logical_not(ring_out[way]))(copy.start)

    def arrive(n, out):
        dist, turn = rounds[n]
        more = dist + 1 < half or (dist + 1 == half and turn == 0)
        for way in range(2):
            def run():
                ring[n][way][1].wait_recv()
                if more:
                    send(n + 2, (way,))
            pl.when(ring_out[way] if out else jnp.logical_not(ring_out[way]))(run)

    count_in = 2 * (lines - 2)
    half_in = count_in // 2

    def place_in(i):
        col = i % 2
        at = i // 2 - 1
        return at * (1 - col) + (count_in - 1 - at) * col

    def index_in(p):
        col = p // half_in
        return 2 * (p * (1 - col) + (count_in - 1 - p) * col + 1) + col

    my_in = (place_in(me_f) + count_in) % count_in
    target_in = (index_in((my_in + 1) % count_in), index_in((my_in + count_in - 1) % count_in))

    def owner_in(way, dist):
        return index_in((my_in + (count_in - dist if way == 0 else dist)) % count_in)

    def mate_of(who):
        at = who // 2
        up = at // (lines // 2)
        return 2 * ((1 - up) * (1 - at) + up * (2 * lines - 3 - at)) + who % 2

    def fold_of(who):
        return jnp.logical_or(who // 2 == 1, who // 2 == lines - 2)

    part_q = deep_q // 2

    def slot_in(head, who, h):
        return wq.at[head, pl.ds(pl.multiple_of(who * deep_q + h * part_q, part_q), part_q), :]

    rounds_in = ring_rounds(half_in)
    per_in = len(rounds_in)
    ring_in = []
    for head in range(heads):
        for s in range(2):
            for dist, turn in rounds_in:
                n = len(ring_in)
                pair_of = []
                for way in range(2):
                    h = half_of(way, turn)
                    gone, come = owner_in(way, dist - 1), owner_in(way, dist)
                    on_out = None if s == 0 or all_fold else fold_of(gone)
                    on_in = None if s == 0 or all_fold else fold_of(come)
                    if s == 1:
                        gone, come = mate_of(gone), mate_of(come)
                    out = remote(slot_in(head, gone, h), slot_in(head, gone, h), fold_send.at[way, n],
                                 fold_recv.at[way, n], (target_in[way], me_t))
                    back = landed(slot_in(head, come, h), fold_send.at[way, n], fold_recv.at[way, n])
                    pair_of.append((out, on_out, back, on_in))
                    started.append((out, inner if on_out is None else jnp.logical_and(inner, on_out)))
                ring_in.append(pair_of)

    def send_in(n):
        for out, on_out, _, _ in ring_in[n]:
            when(on_out, out.start)

    def arrive_in(n):
        for _, _, back, on_in in ring_in[n]:
            when(on_in, back.wait_recv)
        dist, turn = rounds_in[n % per_in]
        if dist + 1 < half_in or (dist + 1 == half_in and turn == 0):
            send_in(n + 2)

    def rows_in(head, who):
        return wq.at[head, pl.ds(pl.multiple_of(who * deep_q, deep_q), deep_q), :]

    puts, puts_in = [], []
    for head in range(heads):
        puts.append(remote(rows_in(head, me_f), rows_in(head, me_f), put_send.at[head], put_recv.at[head],
                           (mate_f, me_t)))
        puts_in.append(landed(rows_in(head, mate_f), put_send.at[head], put_recv.at[head]))
        started.append((puts[-1], is_end))

    up_cols = wu.shape[1]
    deep = wu_ref.shape[0]
    down_rows = wd.shape[1]

    def piece(g, who):
        return wu.at[span(who * deep, deep), :] if g == 0 else wd.at[who]

    def share(g, y):
        if g == 0:
            return wu_ref.at[:, span(y * up_cols, up_cols)]
        return wd_ref.at[span(y * down_rows, down_rows), :]

    line_rounds = [(g, dist, turn) for g in range(2) for dist in range(1, lines) for turn in range(2)]
    per_line = 2 * (lines - 1)

    def line_owner(way, dist, turn):
        at = line - dist if way == 0 else line + dist
        return 2 * at + (pair if turn == 0 else 1 - pair)

    to_end = (line == lines - 2, line == 1)
    line_copies = []
    for m, (g, dist, turn) in enumerate(line_rounds):
        both = []
        for way in range(2):
            who = line_owner(way, dist - 1, turn)
            src = share(g, pair) if dist == 1 and turn == 0 else piece(g, who)
            on = line_next(way) if dist == 1 else jnp.logical_and(line_next(way), line_has(way, dist - 1))
            has = line_has(way, dist)
            if dist == 1 and turn == 1:
                on = jnp.logical_and(on, jnp.logical_not(to_end[way]))
                has = jnp.logical_and(has, inner)
            copy = remote(src, piece(g, who), line_send.at[way, m], line_recv.at[way, m],
                          (step_to(way), me_t))
            back = landed(piece(g, line_owner(way, dist, turn)), line_send.at[way, m],
                          line_recv.at[way, m])
            both.append((copy, on, back, has))
            started.append((copy, on))
        line_copies.append(both)

    def line_send_round(m, ways=(0, 1), out=None):
        for way in ways:
            copy, on, _, _ = line_copies[m][way]
            if out is not None:
                on = jnp.logical_and(on, line_out[way] if out else jnp.logical_not(line_out[way]))
            pl.when(on)(copy.start)

    def line_arrive(m, out):
        g, dist, turn = line_rounds[m]
        for way in range(2):
            def run():
                _, _, back, has = line_copies[m][way]
                pl.when(has)(back.wait_recv)
                if dist + 1 < lines:
                    line_send_round(m + 2, (way,))
            pl.when(line_out[way] if out else jnp.logical_not(line_out[way]))(run)

    aside, aside_in, across_end, across_in = [], [], [], []
    for g in range(2):
        if g == 0:
            stash = xn.at[tokens:tokens + deep, :up_cols]
        else:
            stash = xn.at[tokens:tokens + down_rows, up_cols:up_cols + wd.shape[2]]
        aside.append(remote(share(g, 1 - pair), stash, aside_send.at[g], aside_recv.at[g], (mate_f, me_t)))
        aside_in.append(landed(stash, aside_send.at[g], aside_recv.at[g]))
        across_end.append(remote(stash, piece(g, mate_f), over_send.at[g], over_recv.at[g], (other_f, me_t)))
        across_in.append(landed(piece(g, 2 * mate_line + 1 - pair), over_send.at[g], over_recv.at[g]))
        started.append((aside[-1], folds))
        started.append((across_end[-1], is_end))

    swaps, swaps_in = [], []
    for g in range(2):
        swaps.append(remote(share(g, 1 - pair), piece(g, me_f), swap_send.at[g], swap_recv.at[g],
                            (other_f, me_t)))
        swaps_in.append(landed(piece(g, other_f), swap_send.at[g], swap_recv.at[g]))
        started.append((swaps[-1], None))

    own = [None]
    for n, (src, dst) in enumerate((
            (wo_ref, wo.at[me_f]),
            (share(0, pair), piece(0, me_f)),
            (share(1, pair), piece(1, me_f)))):
        copy = pltpu.make_async_copy(src, dst, own_sem.at[n])
        own.append(copy)

    my_rows = span(me_t * rows, rows)

    def norm(source, gain_ref):
        wide = source.astype(F32)
        mean = jnp.mean(wide * wide, axis=-1, keepdims=True)
        return (wide * lax.rsqrt(mean + EPS) * gain_ref[...]).astype(BF16)

    step = 64

    def norm_into(buf, first, source_ref, gain_ref):
        @pl.loop(0, rows // step)
        def _(i):
            at = pl.multiple_of(i * step, step)
            buf[pl.ds(pl.multiple_of(first + at, step), step), :] = norm(
                source_ref[pl.ds(at, step), :], gain_ref)

    half_rows = rows // 2

    def tok(group, t, part=None):
        first = group * tokens + t * rows
        if part is None:
            return xn.at[span(first, rows), :]
        return xn.at[pl.ds(pl.multiple_of(first + part * half_rows, half_rows), half_rows), :]

    xn_sends = []
    tok_count = [0]

    def tok_pair(out_ref, in_ref, where, on):
        n = tok_count[0]
        tok_count[0] += 1
        out = remote(out_ref, out_ref, tok_send.at[n], tok_recv.at[n], where)
        xn_sends.append((out, on))
        return out, landed(in_ref, tok_send.at[n], tok_recv.at[n])

    def tok_set(group, part, on):
        core_c = tok_pair(tok(group, me_t, part), tok(group, other_t, part), (me_f, other_t), on)
        over, pass_on = [], []
        for e in range(1, chips):
            t = beside(chips - e)
            over.append(tok_pair(tok(group, me_t, part), tok(group, t, part), (me_f, beside(e)), on))
            pass_on.append(tok_pair(
                tok(group, t, part),
                tok(group, 2 * ((chip + chips - e) % chips) + 1 - core, part), (me_f, other_t), on))
        return core_c, over, pass_on

    own_set = tok_set(1, None, inner)
    mate_sets = [tok_set(0, part, folds) for part in range(2)]
    to_mate = [tok_pair(tok(0, me_t, part), tok(0, me_t, part), (mate_f, me_t), is_end) for part in range(2)]

    def tok_start(which):
        which[0][0].start()
        for out, _ in which[1]:
            out.start()

    def tok_pass(which):
        for (_, back), (out, _) in zip(which[1], which[2]):
            back.wait_recv()
            out.start()

    def tok_wait(which):
        which[0][1].wait_recv()
        for _, back in which[2]:
            back.wait_recv()

    def mate_tokens(part):
        def run():
            to_mate[part][1].wait_recv()
            tok_start(mate_sets[part])
        return lambda: when(None if all_fold else folds, run)

    def mate_pass(part):
        return lambda: when(None if all_fold else folds, lambda: tok_pass(mate_sets[part]))

    gates, gates_in = [], []
    for head in range(heads):
        cut = slice(head * DV, (head + 1) * DV)
        gates.append(remote(gated.at[0, :, cut], gated.at[1, :, cut], gate_send.at[head], gate_recv.at[head],
                            (mate_f, me_t)))
        gates_in.append(landed(gated.at[1, :, cut], gate_send.at[head], gate_recv.at[head]))
        started.append((gates[-1], folds))

    def project(group, head):
        width = proj.shape[1]
        t = tile_of(width)

        @pl.loop(0, width // t)
        def _(j):
            cols = pl.ds(pl.multiple_of(j * t, t), t)
            proj[:, cols] = jnp.dot(xn[group * tokens:(group + 1) * tokens, :], wq[head, :, cols],
                                    preferred_element_type=F32).astype(BF16)

    def retain(group, head):
        rate = rate_ref[head]

        @pl.loop(0, tokens // LENGTH)
        def _(n):
            base = pl.multiple_of(n * LENGTH, LENGTH)
            rs = pl.ds(base, LENGTH)
            q = proj[rs, :DK]
            k = proj[rs, DK:2 * DK]
            v = proj[rs, 2 * DK:2 * DK + DV]
            g = proj[rs, 2 * DK + DV:].astype(F32)
            scores = lax.dot_general(q, k, (((1,), (1,)), ((), ())), preferred_element_type=F32)
            t_at = lax.broadcasted_iota(jnp.int32, (LENGTH, LENGTH), 0)
            s_at = lax.broadcasted_iota(jnp.int32, (LENGTH, LENGTH), 1)
            gap = t_at - s_at
            decay = jnp.exp(-rate * jnp.maximum(gap, 0).astype(F32)) * (DK ** -0.5)
            scores = jnp.where(gap >= 0, scores * decay, 0.0).astype(BF16)
            mixed = jnp.dot(scores, v, preferred_element_type=F32)
            mean = jnp.mean(mixed, axis=-1, keepdims=True)
            off = mixed - mean
            var = jnp.mean(off * off, axis=-1, keepdims=True)
            grouped = off * lax.rsqrt(var + EPS)
            gated[group, rs, head * DV:(head + 1) * DV] = (g / (1.0 + jnp.exp(-g)) * grouped).astype(BF16)

    def heads_of(group, head):
        project(group, head)
        retain(group, head)
        if group == 0:
            gates[head].start()

    def mate_heads(head):
        when(None if all_fold else folds, lambda: heads_of(0, head))

    size = rows // chunks

    def mix_block(x, c):
        return part1.at[span((2 * x + c) * rows, rows), :]

    def mix_out():
        cols = wo.shape[2]

        @pl.loop(0, fs)
        def _(j):
            part1[:, span(j * cols, cols)] = jnp.dot(
                gated[1], wo[j], preferred_element_type=F32).astype(BF16)
        order = [e % chips for e in range(1, chips + 1)]
        for e in order:
            x = (chip + e) % chips
            go(remote(mix_block(x, 1 - core), core1.at[e], core1_send.at[e], core1_recv.at[e],
                      (me_f, other_t)))
        for e in order:
            landed(core1.at[e], core1_send.at[e], core1_recv.at[e]).wait_recv()
            if e:
                for c in range(chunks):
                    at = pl.ds(pl.multiple_of(beside(e) * rows + c * size, size), size)
                    here = slice(c * size, (c + 1) * size)
                    more = core1[e, here, :].astype(F32)
                    part1[at, :] = (part1[at, :].astype(F32) + more).astype(BF16)
                    n = (e - 1) * chunks + c
                    go(remote(part1.at[at, :], chip1.at[e - 1, here, :], chip1_send.at[n],
                              chip1_recv.at[n], (me_f, beside(e))))

    def block(y, t):
        return (t % 2) * (2 * chips) + (t // 2) * 2 + y

    def wide(y, t, c):
        return xn2.at[pl.ds(pl.multiple_of(block(y, t) * rows + c * size, size), size), :]

    all_count = [0]

    def all_pair(out_ref, in_ref, where):
        n = all_count[0]
        all_count[0] += 1
        out = remote(out_ref, out_ref, all_send.at[n], all_recv.at[n], where)
        started.append((out, None))
        return out, landed(in_ref, all_send.at[n], all_recv.at[n])

    to_core, to_pair, to_chip, pair_core, chip_core, corner, corner_core = [], [], [], [], [], [], []
    for c in range(chunks):
        to_core.append(all_pair(wide(pair, me_t, c), wide(pair, other_t, c), (me_f, other_t)))
        to_pair.append(all_pair(wide(pair, me_t, c), wide(1 - pair, me_t, c), (other_f, me_t)))
        pair_core.append(all_pair(wide(1 - pair, me_t, c), wide(1 - pair, other_t, c), (me_f, other_t)))
        for found in (to_chip, chip_core, corner, corner_core):
            found.append([])
        for e in range(1, chips):
            t = beside(chips - e)
            t_other = 2 * ((chip + chips - e) % chips) + 1 - core
            to_chip[c].append(all_pair(wide(pair, me_t, c), wide(pair, t, c), (me_f, beside(e))))
            chip_core[c].append(all_pair(wide(pair, t, c), wide(pair, t_other, c), (me_f, other_t)))
            if c < chunks - 1:
                corner[c].append(all_pair(wide(pair, t, c), wide(1 - pair, t, c), (other_f, me_t)))
            else:
                corner[c].append(all_pair(wide(1 - pair, me_t, c), wide(1 - pair, t, c), (me_f, beside(e))))
            corner_core[c].append(all_pair(wide(1 - pair, t, c), wide(1 - pair, t_other, c), (me_f, other_t)))

    def mix_chunk(c):
        here = slice(c * size, (c + 1) * size)
        for e in range(1, chips):
            n = (e - 1) * chunks + c
            landed(chip1.at[e - 1, here, :], chip1_send.at[n], chip1_recv.at[n]).wait_recv()
        total = part1[pl.ds(pl.multiple_of(me_t * rows + c * size, size), size), :].astype(F32)
        total = total + core1[0, here, :].astype(F32)
        for e in range(1, chips):
            total = total + chip1[e - 1, here, :].astype(F32)
        sum_ = (resid_ref[here, :].astype(F32) + total).astype(BF16)
        after[here, :] = sum_
        xn2[pl.ds(pl.multiple_of(block(pair, me_t) * rows + c * size, size), size), :] = norm(
            sum_, mlp_gain_ref)
        to_pair[c][0].start()
        for out, _ in to_chip[c]:
            out.start()
        to_core[c][0].start()

    def take_pair(c):
        to_pair[c][1].wait_recv()
        if c == chunks - 1:
            for out, _ in corner[c]:
                out.start()
        pair_core[c][0].start()

    def take_chip(c):
        for n in range(chips - 1):
            to_chip[c][n][1].wait_recv()
            if c < chunks - 1:
                corner[c][n][0].start()
            chip_core[c][n][0].start()

    def take_corner(c):
        for n in range(chips - 1):
            corner[c][n][1].wait_recv()
            corner_core[c][n][0].start()

    def take_core(found):
        for c in range(chunks):
            for _, back in (found[c] if isinstance(found[c], list) else [found[c]]):
                back.wait_recv()

    def lift(x, y=None):
        t = tile_of(up_cols)
        deep_x = 2 * rows if y is None else rows

        @pl.loop(0, up_cols // t)
        def _(j):
            cols = span(j * t, t)

            @pl.loop(0, 2)
            def _(i):
                at = span(i * tokens + 2 * x * rows + (0 if y is None else y * rows), deep_x)
                up = jnp.maximum(jnp.dot(xn2[at, :], wu[:, cols], preferred_element_type=F32), 0.0)
                hidden[at, cols] = (up * up).astype(BF16)

    cw = wd.shape[2]
    r2 = 2 * chips - 1

    def lower_copy(who, cols, n, ref, where, base=0):
        dst = chip2.at[n, :, cols]
        out = remote(ref, dst, chip2_send.at[base + n, who], chip2_recv.at[base + n, who], where)
        return out, landed(dst, chip2_send.at[base + n, who], chip2_recv.at[base + n, who])

    def part_rows(y, t):
        return span(block(y, t) * rows, rows)

    def along_chips(who, cols):
        first, second = [], []
        for e in range(1, chips):
            for y in range(2):
                first.append(lower_copy(who, cols, 2 * (e - 1) + y, part2.at[part_rows(y, beside(e)), cols],
                                        (me_f, beside(e))))
        second.append(lower_copy(who, cols, r2 - 1, part2.at[part_rows(1 - pair, me_t), cols], (other_f, me_t)))

        def add():
            at = part_rows(1 - pair, me_t)
            total = part2[at, cols].astype(F32)
            for e in range(1, chips):
                total = total + chip2[2 * (e - 1) + 1 - pair, :, cols].astype(F32)
            part2[at, cols] = total.astype(BF16)

        def rest():
            total = chip2[r2 - 1, :, cols].astype(F32)
            for e in range(1, chips):
                total = total + chip2[2 * (e - 1) + pair, :, cols].astype(F32)
            return total
        return first, second, add, rest

    def across_pair(who, cols):
        first, second = [], []
        for e in range(chips):
            first.append(lower_copy(who, cols, e, part2.at[part_rows(1 - pair, beside(e)), cols],
                                    (other_f, me_t), r2))
        for e in range(1, chips):
            second.append(lower_copy(who, cols, chips + e - 1, part2.at[part_rows(pair, beside(e)), cols],
                                     (me_f, beside(e)), r2))

        def add():
            for e in range(1, chips):
                at = part_rows(pair, beside(e))
                part2[at, cols] = (part2[at, cols].astype(F32) + chip2[e, :, cols].astype(F32)).astype(BF16)

        def rest():
            total = chip2[0, :, cols].astype(F32)
            for e in range(1, chips):
                total = total + chip2[chips + e - 1, :, cols].astype(F32)
            return total
        return first, second, add, rest

    finals, joins, middles = [], [], []

    def follow(kind, n, role=None):
        then, on = kind[n]
        if role is not None:
            on = role if on is None else jnp.logical_and(on, role)
        when(on, then)

    J, M = joins, middles
    inner_plan = {1: [(J, 0)], 2: [(J, 1)], 3: [(J, 2)], 4: [(J, 3), (M, 0)], 5: [(J, 4), (J, 5), (M, 1), (M, 2)],
                  6: [(J, 6), (M, 3), (M, 4)], 7: [(J, 7), (M, 5)], None: [(M, 6), (M, 7)]}
    end_plan = {1: [(J, 0)], 2: [(J, 1)], 3: [(J, 2), (J, 3), (M, 0)], 6: [(J, 6), (M, 1), (M, 2)],
                7: [(J, 7), (M, 3)], 8: [(J, 8), (M, 6)], 9: [(J, 9), (M, 7)], None: [(M, 8), (M, 9)]}

    def lower(who, on=None):
        cols = span(who * cw, cw)
        mine = part_rows(pair, me_t)
        side = remote(part2.at[span((1 - core) * tokens, tokens), cols], xn.at[pl.ds(0, tokens), cols],
                      core2_send.at[who], core2_recv.at[who], (me_f, other_t))
        side_in = landed(xn.at[pl.ds(0, tokens), cols], core2_send.at[who], core2_recv.at[who])
        if cw % 256 == 0:
            cuts = [(None, span(who * cw, cw // 2)), (None, span(who * cw + cw // 2, cw // 2))]
        else:
            cuts = [(who % 2 == 0, cols), (who % 2 == 1, cols)]
        plans = [(cuts[0], along_chips(who, cuts[0][1])), (cuts[1], across_pair(who, cuts[1][1]))]

        def run():
            @pl.loop(0, 2)
            def _(i):
                at = span(((1 - core) * (1 - i) + core * i) * tokens, tokens)
                part2[at, cols] = jnp.dot(
                    hidden[at, :], wd[who], preferred_element_type=F32).astype(BF16)

                @pl.when(i == 0)
                def _():
                    side.start()
        def join():
            side_in.wait_recv()

            @pl.loop(0, tokens // 128)
            def _(i):
                at = pl.ds(pl.multiple_of(core * tokens + i * 128, 128), 128)
                more = xn[span(i * 128, 128), cols].astype(F32)
                part2[at, cols] = (part2[at, cols].astype(F32) + more).astype(BF16)
            for (this, _), (first, _, _, _) in plans:
                def begin():
                    for out, _ in first:
                        out.start()
                when(this, begin)

        def middle():
            for (this, _), (first, second, add, _) in plans:
                def pass_on():
                    for _, back in first:
                        back.wait_recv()
                    add()
                    for out, _ in second:
                        out.start()
                when(this, pass_on)

        def end():
            for (this, cut), (first, second, _, rest) in plans:
                def close():
                    for _, back in second:
                        back.wait_recv()
                    total = part2[mine, cut].astype(F32) + rest()
                    out_ref[:, cut] = (after[:, cut].astype(F32) + total).astype(BF16)
                    for out, _ in first + second:
                        out.wait_send()
                when(this, close)
            side.wait_send()

        when(on, run)
        joins.append((join, on))
        middles.append((middle, on))
        finals.append((end, on))
        n = len(middles) - 1
        if all_fold:
            for role, plan in ((inner, inner_plan), (is_end, end_plan)):
                for kind, k in plan.get(n, ()):
                    follow(kind, k, role)
        else:
            follow(joins, n)
            if n >= 2:
                follow(middles, n - 2)

    if all_fold:
        inner_order = [[(0, False), (1, False), (0, True), (1, True)],
                       [(2, False), (3, False), (2, True), (3, True)], [(4, False), (5, False)],
                       [(4, True), (5, True)], [(6, True), (6, False)]]
        end_order = [[(0, False), (1, False), (0, True), (1, True), (2, False), (3, False)],
                     [(2, True), (3, True), (4, False)], [(5, False), (4, True), (5, True), (6, True), (6, False)]]
    else:
        by_round = [(n, out) for n in range(per) for out in (False, True)]
        inner_order = [[], [], [], [], by_round]
        end_order = [[], [], by_round]

    def arrivals(part):
        for n, out in part:
            arrive(n, out)

    def inner_front():
        send(0, out=True)
        send(1, out=True)
        line_send_round(0, out=True)

        when(None if all_fold else folds, aside[0].start)
        line_send_round(per_line, out=True)
        when(None if all_fold else folds, aside[1].start)
        for copy in loads:
            copy.wait()
        send_in(0)
        send_in(1)
        norm_into(xn, tokens + me_t * rows, resid_ref, mix_gain_ref)
        tok_start(own_set)
        for copy in own[1:]:
            copy.start()
        hooks = {(0, 1, 0): mate_tokens(0), (0, 1, 1): lambda: tok_pass(own_set),
                 (1, 0, 0): mate_tokens(1), (1, 0, 2): mate_pass(0), (1, 1, 0): mate_pass(1)}
        order = list(hooks)

        def drain(upto):
            while order and order[0] <= upto:
                hooks[order.pop(0)]()

        for head in range(heads):
            last = head == heads - 1
            first = 2 * head * per_in
            for n in range(per_in):
                arrive_in(first + n)
                drain((head, 0, n))
                if n == 1:
                    if last:
                        send(0, out=False)
                        send(1, out=False)

                    def pushed():
                        puts_in[head].wait_recv()
                    when(None if all_fold else folds, pushed)
                    send_in(first + per_in)
                    send_in(first + per_in + 1)
            for n in range(per_in):
                arrive_in(first + per_in + n)
                if n == 0:
                    if last:
                        for g in range(2):
                            swaps[g].start()
                        arrivals(inner_order[0])
                    else:
                        send_in(first + 2 * per_in)
                        send_in(first + 2 * per_in + 1)
                drain((head, 1, n))
                if n == 0 and last:
                    drain((2, 0, 0))
                    for part in range(2):
                        when(None if all_fold else folds, lambda: tok_wait(mate_sets[part]))
                    for early in range(head):
                        mate_heads(early)
            if not last:
                if head == 0:
                    tok_wait(own_set)
                heads_of(1, head)
        if heads == 1:
            tok_wait(own_set)
        mate_heads(heads - 1)
        arrivals(inner_order[1])
        arrivals(inner_order[2])
        line_send_round(0, out=False)
        heads_of(1, heads - 1)
        arrivals(inner_order[3])
        swaps_in[0].wait_recv()
        line_send_round(1)
        arrivals(inner_order[4])

    def end_front():
        send(0, out=True)
        send(1, out=True)
        for g in range(2):
            swaps[g].start()
        for copy in loads:
            copy.wait()
        puts[0].start()
        norm_into(xn, me_t * rows, resid_ref, mix_gain_ref)
        for out, _ in to_mate:
            out.start()
        for head in range(1, heads):
            puts[head].start()
        send(0, out=False)
        send(1, out=False)
        for copy in own[1:]:
            copy.start()
        arrivals(end_order[0])
        swaps_in[0].wait_recv()
        aside_in[0].wait_recv()
        across_end[0].start()
        line_send_round(0)
        arrivals(end_order[1])
        line_send_round(1)
        aside_in[1].wait_recv()
        across_end[1].start()
        line_send_round(per_line)
        swaps_in[1].wait_recv()
        line_send_round(per_line + 1)
        arrivals(end_order[2])
        for back in gates_in:
            back.wait_recv()

    pl.when(inner)(inner_front)
    pl.when(is_end)(end_front)
    own[1].wait()
    mix_out()
    line_arrive(0, False)
    line_arrive(1, False)

    def inner_down():
        line_send_round(per_line, out=False)
        swaps_in[1].wait_recv()
        line_send_round(per_line + 1)
    pl.when(inner)(inner_down)

    line_arrive(0, True)
    for copy, on in xn_sends:
        pl.when(on)(copy.wait_send)
    for c in range(chunks):
        mix_chunk(c)
        if c == 3:
            line_arrive(1, True)
        if c > 1:
            take_pair(c - 2)
    line_arrive(2, False)
    line_arrive(3, False)
    line_arrive(2, True)
    for c in range(chunks - 2, chunks):
        take_pair(c)
    for c in range(chunks // 2):
        if c == chunks // 4:
            line_arrive(3, True)
        take_chip(c)
    for k in range(4, per_line):
        line_arrive(k, False)
        line_arrive(k, True)
    for k in range(2):
        line_arrive(per_line + k, False)

    def end_landed():
        for back in across_in:
            back.wait_recv()
    pl.when(is_end)(end_landed)
    own[2].wait()
    own[3].wait()
    take_core(to_core)
    take_core(pair_core)
    for c in range(chunks // 2, chunks):
        take_chip(c)
        take_corner(c - chunks // 2)
        if c == chunks // 2:
            lift(chip, pair)
        elif c == chunks // 2 + 1:
            lift(chip, 1 - pair)
    line_arrive(per_line, True)
    take_core(chip_core)
    for e in range(1, chips):
        lift((chip + e) % chips, pair)
    for c in range(chunks // 2, chunks):
        take_corner(c)
    take_core(corner_core)
    for e in range(1, chips):
        lift((chip + e) % chips, 1 - pair)
    line_arrive(per_line + 1, True)
    inward = range(1, lines // 2)
    blocks = [None, None]
    for dist in range(1, lines):
        first = per_line + 2 * (dist - 1)
        for out in (True, False):
            if out or dist in inward:
                blocks += [(first, out), (first + 1, out)]
    for n, this in enumerate(blocks):
        if this is None:
            lower(me_f if n == 0 else other_f)
            continue
        m, out = this
        _, dist, turn = line_rounds[m]
        if all_fold:
            if n == 2:
                pl.when(inner)(lambda: line_arrive(per_line + 2, True))
            elif n == 5:
                pl.when(inner)(lambda: line_arrive(per_line + 3, True))
            if dist == 2:
                pl.when(is_end)(lambda: line_arrive(m, True))
            elif dist > 2:
                line_arrive(m, True)
        elif dist > 1:
            line_arrive(m, out)
        at = line + dist - 2 * dist * upper if out else line - dist + 2 * dist * upper
        has = jnp.logical_and(at >= 0, at <= lines - 1)
        if not out:
            has = jnp.logical_and(has, at // (lines // 2) == upper)
        lower(2 * at + (pair if turn == 0 else 1 - pair), has)

    if all_fold:
        for role, plan in ((inner, inner_plan), (is_end, end_plan)):
            for kind, k in plan[None]:
                follow(kind, k, role)
    else:
        for n in range(len(middles) - 2, len(middles)):
            follow(middles, n)
    for end, on in finals:
        when(on, end)
    for copy, on in started:
        when(on, copy.wait_send)


def on_device(fs, tp, resid, mix_gain, w_query, w_key, w_value, w_gate, w_output, decay_rate,
              mlp_gain, w_up, w_down):
    rows, width = resid.shape
    tokens = rows * tp
    in_width = w_query.shape[1] + w_key.shape[1] + w_value.shape[1] + w_gate.shape[1]
    chips = tp // 2
    heads = decay_rate.shape[0]
    wide = CHUNKS * (3 + 4 * (chips - 1))
    vmem = pl.BlockSpec(memory_space=pltpu.VMEM)
    hbm = pl.BlockSpec(memory_space=pl.ANY)
    dma = pltpu.SemaphoreType.DMA
    cols = width // fs
    return pl.pallas_call(
        functools.partial(kernel, fs, tp),
        out_shape=jax.ShapeDtypeStruct((rows, width), BF16),
        in_specs=[vmem] * 3 + [pl.BlockSpec(memory_space=pltpu.SMEM)] + [hbm] * 7,
        out_specs=vmem,
        scratch_shapes=[
            pltpu.VMEM((heads, width, in_width // heads), BF16),
            pltpu.VMEM((fs, w_output.shape[0], cols), BF16),
            pltpu.VMEM((width, w_up.shape[1] // 2), BF16),
            pltpu.VMEM((fs, w_down.shape[0] // 2, cols), BF16),
            pltpu.VMEM((2 * tokens, width), BF16),
            pltpu.VMEM((2 * tokens, width), BF16),
            pltpu.VMEM((tokens, in_width // heads), BF16),
            pltpu.VMEM((2, tokens, w_output.shape[0]), BF16),
            pltpu.VMEM((2 * tokens, w_up.shape[1] // 2), BF16),
            pltpu.VMEM((tokens, width), BF16),
            pltpu.VMEM((chips, rows, width), BF16),
            pltpu.VMEM((chips - 1, rows, width), BF16),
            pltpu.VMEM((2 * tokens, width), BF16),
            pltpu.VMEM((2 * chips - 1, rows, width), BF16),
            pltpu.VMEM((rows, width), BF16),
            dma((2, fs - 1)),
            dma((2, fs - 1)),
            dma((3,)),
            dma((4 * heads,)),
            dma((2, 2 * heads * (fs - 5))),
            dma((2, 2 * heads * (fs - 5))),
            dma((heads,)),
            dma((heads,)),
            dma((3 * (2 * chips - 1) + 2,)),
            dma((3 * (2 * chips - 1) + 2,)),
            dma((heads,)),
            dma((heads,)),
            dma((2,)),
            dma((2,)),
            dma((2,)),
            dma((2,)),
            dma((2, 2 * (fs - 2))),
            dma((2, 2 * (fs - 2))),
            dma((2,)),
            dma((2,)),
            dma((chips,)),
            dma((chips,)),
            dma((CHUNKS * (chips - 1),)),
            dma((CHUNKS * (chips - 1),)),
            dma((wide,)),
            dma((wide,)),
            dma((fs,)),
            dma((fs,)),
            dma((2 * (2 * chips - 1), fs)),
            dma((2 * (2 * chips - 1), fs)),
        ],
        compiler_params=pltpu.CompilerParams(
            collective_id=0, has_side_effects=True, vmem_limit_bytes=67043328),
    )(resid, mix_gain[None, :], mlp_gain[None, :], decay_rate, w_query, w_key, w_value,
      w_gate, w_output, w_up, w_down)


def solution(mesh):
    placed = (
        P(("fs", "tp"), None),
        P(),
        P("fs", "tp"),
        P("fs", "tp"),
        P("fs", "tp"),
        P("fs", "tp"),
        P("tp", "fs"),
        P("tp"),
        P(),
        P("fs", "tp"),
        P("tp", "fs"),
    )
    sizes = dict(mesh.shape)
    return jax.shard_map(
        functools.partial(on_device, sizes["fs"], sizes["tp"]), mesh=mesh, in_specs=placed,
        out_specs=P(("fs", "tp"), None), check_vma=False)
```

```python
import functools

import jax
import jax.numpy as jnp
from jax import lax
from jax.experimental import pallas as pl
from jax.experimental.pallas import tpu as pltpu
from jax.sharding import PartitionSpec as P

DK = 128
DV = 256
LENGTH = 512
MESH = pl.DeviceIdType.MESH
EPS = 1e-06
CHUNKS = 8
F32 = jnp.float32
BF16 = jnp.bfloat16


def tile_of(width):
    return 256 if width % 256 == 0 else 128


def kernel(fs, tp, resid_hbm, mix_gain_hbm, mlp_gain_hbm, rate_ref, w1_ref, w2_ref, w3_ref, w4_ref, wo_ref, wu_ref, wd_ref,
           out_ref, resid_ref, mix_gain_ref, mlp_gain_ref, load_sem, out_sem, wq, wo, wu, wd, xn, xn2, proj, gated, hidden, part1, core1, chip1, part2, chip2,
           after, ring_send, ring_recv, own_sem, in_sem, fold_send, fold_recv, put_send, put_recv,
           tok_send, tok_recv, gate_send, gate_recv, aside_send, aside_recv, over_send, over_recv, line_send, line_recv,
           swap_send, swap_recv, core1_send, core1_recv, chip1_send, chip1_recv, all_send, all_recv,
           core2_send, core2_recv, chip2_send, chip2_recv):
    half = fs // 2
    lines = fs // 2
    chunks = CHUNKS
    in_refs = (w1_ref, w2_ref, w3_ref, w4_ref)
    deep_q = w1_ref.shape[0]
    chips = tp // 2
    rows = resid_hbm.shape[0]
    heads = rate_ref.shape[0]
    tokens = rows * tp
    me_f = lax.axis_index("fs")
    me_t = lax.axis_index("tp")
    pair = me_f % 2
    line = me_f // 2
    other_f = 2 * line + 1 - pair
    chip = me_t // 2
    core = me_t % 2
    other_t = 2 * chip + 1 - core

    def place(i):
        col = i % 2
        at = i // 2
        return at * (1 - col) + (fs - 1 - at) * col

    def index(p):
        col = p // half
        return 2 * (p * (1 - col) + (fs - 1 - p) * col) + col

    my_place = place(me_f)
    target = (index((my_place + 1) % fs), index((my_place + fs - 1) % fs))

    def owner(way, dist):
        if way == 0:
            return index((my_place + fs - dist) % fs)
        return index((my_place + dist) % fs)

    def peer(d):
        return (me_t + d) % tp

    def beside(e):
        return 2 * ((chip + e) % chips) + core

    def step_to(way):
        return me_f + 2 if way == 0 else me_f - 2

    def line_has(way, dist):
        return line >= dist if way == 0 else line + dist <= lines - 1

    def line_next(way):
        return line_has(1 - way, 1)

    upper = line // (lines // 2)
    mate_line = (1 - upper) * (1 - line) + upper * (2 * lines - 3 - line)
    mate_f = 2 * mate_line + pair
    all_fold = lines - 2 == 2
    is_end = jnp.logical_or(line == 0, line == lines - 1)
    inner = jnp.logical_not(is_end)
    folds = inner if all_fold else jnp.logical_or(line == 1, line == lines - 2)
    ring_out = (upper + pair == 1, upper + pair != 1)
    line_out = (upper == 1, upper == 0)

    def when(on, run):
        if on is None:
            run()
        else:
            pl.when(on)(run)

    first_row = pl.multiple_of(me_f * deep_q, deep_q)
    loads = []
    for head in range(heads):
        left = 0
        for ref in in_refs:
            w = ref.shape[1] // heads
            copy = pltpu.make_async_copy(
                ref.at[:, head * w:(head + 1) * w],
                wq.at[head, pl.ds(first_row, deep_q), left:left + w], in_sem.at[len(loads)])
            copy.start()
            loads.append(copy)
            left += w

    row_loads = []
    for n, (src, dst) in enumerate(((resid_hbm, resid_ref), (mix_gain_hbm, mix_gain_ref),
                                    (mlp_gain_hbm, mlp_gain_ref))):
        copy = pltpu.make_async_copy(src, dst, load_sem.at[n])
        copy.start()
        row_loads.append(copy)

    barrier = pltpu.get_barrier_semaphore()

    def greet(where):
        pl.semaphore_signal(barrier, inc=1, device_id=where, device_id_type=MESH)

    for way in range(2):
        greet((target[way], me_t))
    for d in range(1, tp):
        greet((me_f, peer(d)))
        if d % 2 == 0:
            greet((other_f, peer(d)))
    greet((other_f, me_t))
    for way in range(2):
        at = (line + (1 if way == 0 else lines - 1)) % lines
        greet((2 * at + pair, me_t))
    pl.semaphore_wait(barrier, 2 + (tp - 1) + (chips - 1) + 1 + 2)

    started = []

    def go(copy, on=None):
        if on is None:
            copy.start()
        else:
            @pl.when(on)
            def _():
                copy.start()
        started.append((copy, on))

    def remote(src, dst, s_sem, r_sem, where):
        return pltpu.make_async_remote_copy(
            src_ref=src, dst_ref=dst, send_sem=s_sem, recv_sem=r_sem, device_id=where,
            device_id_type=MESH)

    def landed(dst, s_sem, r_sem):
        return remote(dst, dst, s_sem, r_sem, (me_f, other_t))

    def span(at, size):
        return pl.ds(pl.multiple_of(at, size), size)

    def half_of(way, turn):
        return turn if way == 0 else 1 - turn

    def ring_rounds(half_ring):
        found = []
        for dist in range(1, half_ring):
            found += [(dist, 0), (dist, 1)]
        return found + [(half_ring, 0)]

    rounds = ring_rounds(half)
    per = len(rounds)
    out_rows = wo_ref.shape[0] // 2

    def slot(who, h):
        return wo.at[who, pl.ds(h * out_rows, out_rows), :]

    ring = []
    for n, (dist, turn) in enumerate(rounds):
        pair_of = []
        for way in range(2):
            h = half_of(way, turn)
            who = owner(way, dist - 1)
            src = wo_ref.at[pl.ds(h * out_rows, out_rows), :] if dist == 1 else slot(who, h)
            pair_of.append((
                remote(src, slot(who, h), ring_send.at[way, n], ring_recv.at[way, n], (target[way], me_t)),
                landed(slot(owner(way, dist), h), ring_send.at[way, n], ring_recv.at[way, n])))
            started.append((pair_of[-1][0], None))
        ring.append(pair_of)

    def send(n, ways=(0, 1), out=None):
        for way in ways:
            copy = ring[n][way][0]
            if out is None:
                copy.start()
            else:
                pl.when(ring_out[way] if out else jnp.logical_not(ring_out[way]))(copy.start)

    def arrive(n, out):
        dist, turn = rounds[n]
        more = dist + 1 < half or (dist + 1 == half and turn == 0)
        for way in range(2):
            def run():
                ring[n][way][1].wait_recv()
                if more:
                    send(n + 2, (way,))
            pl.when(ring_out[way] if out else jnp.logical_not(ring_out[way]))(run)

    count_in = 2 * (lines - 2)
    half_in = count_in // 2

    def place_in(i):
        col = i % 2
        at = i // 2 - 1
        return at * (1 - col) + (count_in - 1 - at) * col

    def index_in(p):
        col = p // half_in
        return 2 * (p * (1 - col) + (count_in - 1 - p) * col + 1) + col

    my_in = (place_in(me_f) + count_in) % count_in
    target_in = (index_in((my_in + 1) % count_in), index_in((my_in + count_in - 1) % count_in))

    def owner_in(way, dist):
        return index_in((my_in + (count_in - dist if way == 0 else dist)) % count_in)

    def mate_of(who):
        at = who // 2
        up = at // (lines // 2)
        return 2 * ((1 - up) * (1 - at) + up * (2 * lines - 3 - at)) + who % 2

    def fold_of(who):
        return jnp.logical_or(who // 2 == 1, who // 2 == lines - 2)

    part_q = deep_q // 2

    def slot_in(head, who, h):
        return wq.at[head, pl.ds(pl.multiple_of(who * deep_q + h * part_q, part_q), part_q), :]

    rounds_in = ring_rounds(half_in)
    per_in = len(rounds_in)
    ring_in = []
    for head in range(heads):
        for s in range(2):
            for dist, turn in rounds_in:
                n = len(ring_in)
                pair_of = []
                for way in range(2):
                    h = half_of(way, turn)
                    gone, come = owner_in(way, dist - 1), owner_in(way, dist)
                    on_out = None if s == 0 or all_fold else fold_of(gone)
                    on_in = None if s == 0 or all_fold else fold_of(come)
                    if s == 1:
                        gone, come = mate_of(gone), mate_of(come)
                    out = remote(slot_in(head, gone, h), slot_in(head, gone, h), fold_send.at[way, n],
                                 fold_recv.at[way, n], (target_in[way], me_t))
                    back = landed(slot_in(head, come, h), fold_send.at[way, n], fold_recv.at[way, n])
                    pair_of.append((out, on_out, back, on_in))
                    started.append((out, inner if on_out is None else jnp.logical_and(inner, on_out)))
                ring_in.append(pair_of)

    def send_in(n):
        for out, on_out, _, _ in ring_in[n]:
            when(on_out, out.start)

    def arrive_in(n):
        for _, _, back, on_in in ring_in[n]:
            when(on_in, back.wait_recv)
        dist, turn = rounds_in[n % per_in]
        if dist + 1 < half_in or (dist + 1 == half_in and turn == 0):
            send_in(n + 2)

    def rows_in(head, who):
        return wq.at[head, pl.ds(pl.multiple_of(who * deep_q, deep_q), deep_q), :]

    puts, puts_in = [], []
    for head in range(heads):
        puts.append(remote(rows_in(head, me_f), rows_in(head, me_f), put_send.at[head], put_recv.at[head],
                           (mate_f, me_t)))
        puts_in.append(landed(rows_in(head, mate_f), put_send.at[head], put_recv.at[head]))
        started.append((puts[-1], is_end))

    up_cols = wu.shape[1]
    deep = wu_ref.shape[0]
    down_rows = wd.shape[1]

    def piece(g, who):
        return wu.at[span(who * deep, deep), :] if g == 0 else wd.at[who]

    def share(g, y):
        if g == 0:
            return wu_ref.at[:, span(y * up_cols, up_cols)]
        return wd_ref.at[span(y * down_rows, down_rows), :]

    line_rounds = [(g, dist, turn) for g in range(2) for dist in range(1, lines) for turn in range(2)]
    per_line = 2 * (lines - 1)

    def line_owner(way, dist, turn):
        at = line - dist if way == 0 else line + dist
        return 2 * at + (pair if turn == 0 else 1 - pair)

    to_end = (line == lines - 2, line == 1)
    line_copies = []
    for m, (g, dist, turn) in enumerate(line_rounds):
        both = []
        for way in range(2):
            who = line_owner(way, dist - 1, turn)
            src = share(g, pair) if dist == 1 and turn == 0 else piece(g, who)
            on = line_next(way) if dist == 1 else jnp.logical_and(line_next(way), line_has(way, dist - 1))
            has = line_has(way, dist)
            if dist == 1 and turn == 1:
                on = jnp.logical_and(on, jnp.logical_not(to_end[way]))
                has = jnp.logical_and(has, inner)
            copy = remote(src, piece(g, who), line_send.at[way, m], line_recv.at[way, m],
                          (step_to(way), me_t))
            back = landed(piece(g, line_owner(way, dist, turn)), line_send.at[way, m],
                          line_recv.at[way, m])
            both.append((copy, on, back, has))
            started.append((copy, on))
        line_copies.append(both)

    def line_send_round(m, ways=(0, 1), out=None):
        for way in ways:
            copy, on, _, _ = line_copies[m][way]
            if out is not None:
                on = jnp.logical_and(on, line_out[way] if out else jnp.logical_not(line_out[way]))
            pl.when(on)(copy.start)

    def line_arrive(m, out):
        g, dist, turn = line_rounds[m]
        for way in range(2):
            def run():
                _, _, back, has = line_copies[m][way]
                pl.when(has)(back.wait_recv)
                if dist + 1 < lines:
                    line_send_round(m + 2, (way,))
            pl.when(line_out[way] if out else jnp.logical_not(line_out[way]))(run)

    aside, aside_in, across_end, across_in = [], [], [], []
    for g in range(2):
        if g == 0:
            stash = xn.at[tokens:tokens + deep, :up_cols]
        else:
            stash = xn.at[tokens:tokens + down_rows, up_cols:up_cols + wd.shape[2]]
        aside.append(remote(share(g, 1 - pair), stash, aside_send.at[g], aside_recv.at[g], (mate_f, me_t)))
        aside_in.append(landed(stash, aside_send.at[g], aside_recv.at[g]))
        across_end.append(remote(stash, piece(g, mate_f), over_send.at[g], over_recv.at[g], (other_f, me_t)))
        across_in.append(landed(piece(g, 2 * mate_line + 1 - pair), over_send.at[g], over_recv.at[g]))
        started.append((aside[-1], folds))
        started.append((across_end[-1], is_end))

    swaps, swaps_in = [], []
    for g in range(2):
        swaps.append(remote(share(g, 1 - pair), piece(g, me_f), swap_send.at[g], swap_recv.at[g],
                            (other_f, me_t)))
        swaps_in.append(landed(piece(g, other_f), swap_send.at[g], swap_recv.at[g]))
        started.append((swaps[-1], None))

    own = [None]
    for n, (src, dst) in enumerate((
            (wo_ref, wo.at[me_f]),
            (share(0, pair), piece(0, me_f)),
            (share(1, pair), piece(1, me_f)))):
        copy = pltpu.make_async_copy(src, dst, own_sem.at[n])
        own.append(copy)

    my_rows = span(me_t * rows, rows)

    def norm(source, gain_ref):
        wide = source.astype(F32)
        mean = jnp.mean(wide * wide, axis=-1, keepdims=True)
        return (wide * lax.rsqrt(mean + EPS) * gain_ref[...]).astype(BF16)

    step = 64

    def norm_into(buf, first, source_ref, gain_ref):
        @pl.loop(0, rows // step)
        def _(i):
            at = pl.multiple_of(i * step, step)
            buf[pl.ds(pl.multiple_of(first + at, step), step), :] = norm(
                source_ref[pl.ds(at, step), :], gain_ref)

    half_rows = rows // 2

    def tok(group, t, part=None):
        first = group * tokens + t * rows
        if part is None:
            return xn.at[span(first, rows), :]
        return xn.at[pl.ds(pl.multiple_of(first + part * half_rows, half_rows), half_rows), :]

    xn_sends = []
    tok_count = [0]

    def tok_pair(out_ref, in_ref, where, on):
        n = tok_count[0]
        tok_count[0] += 1
        out = remote(out_ref, out_ref, tok_send.at[n], tok_recv.at[n], where)
        xn_sends.append((out, on))
        return out, landed(in_ref, tok_send.at[n], tok_recv.at[n])

    def tok_set(group, part, on):
        core_c = tok_pair(tok(group, me_t, part), tok(group, other_t, part), (me_f, other_t), on)
        over, pass_on = [], []
        for e in range(1, chips):
            t = beside(chips - e)
            over.append(tok_pair(tok(group, me_t, part), tok(group, t, part), (me_f, beside(e)), on))
            pass_on.append(tok_pair(
                tok(group, t, part),
                tok(group, 2 * ((chip + chips - e) % chips) + 1 - core, part), (me_f, other_t), on))
        return core_c, over, pass_on

    own_set = tok_set(1, None, inner)
    mate_sets = [tok_set(0, part, folds) for part in range(2)]
    to_mate = [tok_pair(tok(0, me_t, part), tok(0, me_t, part), (mate_f, me_t), is_end) for part in range(2)]

    def tok_start(which):
        which[0][0].start()
        for out, _ in which[1]:
            out.start()

    def tok_pass(which):
        for (_, back), (out, _) in zip(which[1], which[2]):
            back.wait_recv()
            out.start()

    def tok_wait(which):
        which[0][1].wait_recv()
        for _, back in which[2]:
            back.wait_recv()

    def mate_tokens(part):
        def run():
            to_mate[part][1].wait_recv()
            tok_start(mate_sets[part])
        return lambda: when(None if all_fold else folds, run)

    def mate_pass(part):
        return lambda: when(None if all_fold else folds, lambda: tok_pass(mate_sets[part]))

    gates, gates_in = [], []
    for head in range(heads):
        cut = slice(head * DV, (head + 1) * DV)
        gates.append(remote(gated.at[0, :, cut], gated.at[1, :, cut], gate_send.at[head], gate_recv.at[head],
                            (mate_f, me_t)))
        gates_in.append(landed(gated.at[1, :, cut], gate_send.at[head], gate_recv.at[head]))
        started.append((gates[-1], folds))

    def project(group, head):
        width = proj.shape[1]
        t = tile_of(width)

        @pl.loop(0, width // t)
        def _(j):
            cols = pl.ds(pl.multiple_of(j * t, t), t)
            proj[:, cols] = jnp.dot(xn[group * tokens:(group + 1) * tokens, :], wq[head, :, cols],
                                    preferred_element_type=F32).astype(BF16)

    def retain(group, head):
        rate = rate_ref[head]

        @pl.loop(0, tokens // LENGTH)
        def _(n):
            base = pl.multiple_of(n * LENGTH, LENGTH)
            rs = pl.ds(base, LENGTH)
            q = proj[rs, :DK]
            k = proj[rs, DK:2 * DK]
            v = proj[rs, 2 * DK:2 * DK + DV]
            g = proj[rs, 2 * DK + DV:].astype(F32)
            scores = lax.dot_general(q, k, (((1,), (1,)), ((), ())), preferred_element_type=F32)
            t_at = lax.broadcasted_iota(jnp.int32, (LENGTH, LENGTH), 0)
            s_at = lax.broadcasted_iota(jnp.int32, (LENGTH, LENGTH), 1)
            gap = t_at - s_at
            decay = jnp.exp(-rate * jnp.maximum(gap, 0).astype(F32)) * (DK ** -0.5)
            scores = jnp.where(gap >= 0, scores * decay, 0.0).astype(BF16)
            mixed = jnp.dot(scores, v, preferred_element_type=F32)
            mean = jnp.mean(mixed, axis=-1, keepdims=True)
            off = mixed - mean
            var = jnp.mean(off * off, axis=-1, keepdims=True)
            grouped = off * lax.rsqrt(var + EPS)
            gated[group, rs, head * DV:(head + 1) * DV] = (g / (1.0 + jnp.exp(-g)) * grouped).astype(BF16)

    def heads_of(group, head):
        project(group, head)
        retain(group, head)
        if group == 0:
            gates[head].start()

    def mate_heads(head):
        when(None if all_fold else folds, lambda: heads_of(0, head))

    size = rows // chunks

    def mix_out():
        cols = wo.shape[2]

        order = [e % chips for e in range(1, chips + 1)]
        wide_half = part1.shape[1] // 2

        def to_other(e, part):
            cut = slice(part * wide_half, (part + 1) * wide_half)
            at = span((2 * ((chip + e) % chips) + 1 - core) * rows, rows)
            n = 2 * e + part
            return (part1.at[at, cut], core1.at[e, :, cut], core1_send.at[n], core1_recv.at[n])

        for part in range(2):
            @pl.loop(0, fs // 2)
            def _(i):
                j = i + part * (fs // 2)
                part1[:, span(j * cols, cols)] = jnp.dot(
                    gated[1], wo[j], preferred_element_type=F32).astype(BF16)
            for e in order:
                go(remote(*to_other(e, part), (me_f, other_t)))
        for e in order:
            for part in range(2):
                _, dst, s_sem, r_sem = to_other(e, part)
                landed(dst, s_sem, r_sem).wait_recv()
            if e:
                for c in range(chunks):
                    at = pl.ds(pl.multiple_of(beside(e) * rows + c * size, size), size)
                    here = slice(c * size, (c + 1) * size)
                    more = core1[e, here, :].astype(F32)
                    part1[at, :] = (part1[at, :].astype(F32) + more).astype(BF16)
                    n = (e - 1) * chunks + c
                    go(remote(part1.at[at, :], chip1.at[e - 1, here, :], chip1_send.at[n],
                              chip1_recv.at[n], (me_f, beside(e))))

    def block(y, t):
        return (t % 2) * (2 * chips) + (t // 2) * 2 + y

    def wide(y, t, c):
        return xn2.at[pl.ds(pl.multiple_of(block(y, t) * rows + c * size, size), size), :]

    all_count = [0]

    def all_pair(out_ref, in_ref, where):
        n = all_count[0]
        all_count[0] += 1
        out = remote(out_ref, out_ref, all_send.at[n], all_recv.at[n], where)
        started.append((out, None))
        return out, landed(in_ref, all_send.at[n], all_recv.at[n])

    to_core, to_pair, to_chip, pair_core, chip_core, corner, corner_core = [], [], [], [], [], [], []
    for c in range(chunks):
        to_core.append(all_pair(wide(pair, me_t, c), wide(pair, other_t, c), (me_f, other_t)))
        to_pair.append(all_pair(wide(pair, me_t, c), wide(1 - pair, me_t, c), (other_f, me_t)))
        pair_core.append(all_pair(wide(1 - pair, me_t, c), wide(1 - pair, other_t, c), (me_f, other_t)))
        for found in (to_chip, chip_core, corner, corner_core):
            found.append([])
        for e in range(1, chips):
            t = beside(chips - e)
            t_other = 2 * ((chip + chips - e) % chips) + 1 - core
            to_chip[c].append(all_pair(wide(pair, me_t, c), wide(pair, t, c), (me_f, beside(e))))
            chip_core[c].append(all_pair(wide(pair, t, c), wide(pair, t_other, c), (me_f, other_t)))
            if c < chunks - 1:
                corner[c].append(all_pair(wide(pair, t, c), wide(1 - pair, t, c), (other_f, me_t)))
            else:
                corner[c].append(all_pair(wide(1 - pair, me_t, c), wide(1 - pair, t, c), (me_f, beside(e))))
            corner_core[c].append(all_pair(wide(1 - pair, t, c), wide(1 - pair, t_other, c), (me_f, other_t)))

    def mix_chunk(c):
        here = slice(c * size, (c + 1) * size)
        for e in range(1, chips):
            n = (e - 1) * chunks + c
            landed(chip1.at[e - 1, here, :], chip1_send.at[n], chip1_recv.at[n]).wait_recv()
        total = part1[pl.ds(pl.multiple_of(me_t * rows + c * size, size), size), :].astype(F32)
        total = total + core1[0, here, :].astype(F32)
        for e in range(1, chips):
            total = total + chip1[e - 1, here, :].astype(F32)
        sum_ = (resid_ref[here, :].astype(F32) + total).astype(BF16)
        after[here, :] = sum_
        xn2[pl.ds(pl.multiple_of(block(pair, me_t) * rows + c * size, size), size), :] = norm(
            sum_, mlp_gain_ref)
        to_pair[c][0].start()
        for out, _ in to_chip[c]:
            out.start()
        to_core[c][0].start()

    def take_pair(c):
        to_pair[c][1].wait_recv()
        if c == chunks - 1:
            for out, _ in corner[c]:
                out.start()
        pair_core[c][0].start()

    def take_chip(c):
        for n in range(chips - 1):
            to_chip[c][n][1].wait_recv()
            if c < chunks - 1:
                corner[c][n][0].start()
            chip_core[c][n][0].start()

    def take_corner(c):
        for n in range(chips - 1):
            corner[c][n][1].wait_recv()
            corner_core[c][n][0].start()

    def take_core(found):
        for c in range(chunks):
            for _, back in (found[c] if isinstance(found[c], list) else [found[c]]):
                back.wait_recv()

    def lift(x, y, cores):
        t = tile_of(up_cols)

        @pl.loop(0, up_cols // t)
        def _(j):
            cols = span(j * t, t)
            for c in cores:
                at = span(c * tokens + (2 * x + y) * rows, rows)
                up = jnp.maximum(jnp.dot(xn2[at, :], wu[:, cols], preferred_element_type=F32), 0.0)
                hidden[at, cols] = (up * up).astype(BF16)

    cw = wd.shape[2]
    r2 = 2 * chips - 1

    def lower_copy(who, cols, n, ref, where, base=0):
        dst = chip2.at[n, :, cols]
        out = remote(ref, dst, chip2_send.at[base + n, who], chip2_recv.at[base + n, who], where)
        return out, landed(dst, chip2_send.at[base + n, who], chip2_recv.at[base + n, who])

    def part_rows(y, t):
        return span(block(y, t) * rows, rows)

    def along_chips(who, cols):
        first, second = [], []
        for e in range(1, chips):
            for y in range(2):
                first.append(lower_copy(who, cols, 2 * (e - 1) + y, part2.at[part_rows(y, beside(e)), cols],
                                        (me_f, beside(e))))
        second.append(lower_copy(who, cols, r2 - 1, part2.at[part_rows(1 - pair, me_t), cols], (other_f, me_t)))

        def add():
            at = part_rows(1 - pair, me_t)
            total = part2[at, cols].astype(F32)
            for e in range(1, chips):
                total = total + chip2[2 * (e - 1) + 1 - pair, :, cols].astype(F32)
            part2[at, cols] = total.astype(BF16)

        def rest():
            total = chip2[r2 - 1, :, cols].astype(F32)
            for e in range(1, chips):
                total = total + chip2[2 * (e - 1) + pair, :, cols].astype(F32)
            return total
        return first, second, add, rest

    def across_pair(who, cols):
        first, second = [], []
        for e in range(chips):
            first.append(lower_copy(who, cols, e, part2.at[part_rows(1 - pair, beside(e)), cols],
                                    (other_f, me_t), r2))
        for e in range(1, chips):
            second.append(lower_copy(who, cols, chips + e - 1, part2.at[part_rows(pair, beside(e)), cols],
                                     (me_f, beside(e)), r2))

        def add():
            for e in range(1, chips):
                at = part_rows(pair, beside(e))
                part2[at, cols] = (part2[at, cols].astype(F32) + chip2[e, :, cols].astype(F32)).astype(BF16)

        def rest():
            total = chip2[0, :, cols].astype(F32)
            for e in range(1, chips):
                total = total + chip2[chips + e - 1, :, cols].astype(F32)
            return total
        return first, second, add, rest

    finals, joins, middles, giving = [], [], [], []

    def follow(kind, n, role=None):
        then, on = kind[n]
        if role is not None:
            on = role if on is None else jnp.logical_and(on, role)
        when(on, then)

    J, M = joins, middles
    inner_plan = {1: [(J, 0)], 2: [(J, 1)], 3: [(J, 2)], 4: [(J, 3), (M, 0)], 5: [(J, 4), (J, 5), (M, 1), (M, 2)],
                  6: [(J, 6), (M, 3), (M, 4)], 7: [(J, 7), (M, 5)], None: [(M, 6), (M, 7)]}
    end_plan = {1: [(J, 0)], 2: [(J, 1)], 3: [(J, 2), (J, 3), (M, 0)], 6: [(J, 6), (M, 1), (M, 2)],
                7: [(J, 7), (M, 3)], 8: [(J, 8), (M, 6)], 9: [(J, 9), (M, 7)], None: [(M, 8), (M, 9)]}

    def lower(who, on=None):
        cols = span(who * cw, cw)
        mine = part_rows(pair, me_t)
        side = remote(part2.at[span((1 - core) * tokens, tokens), cols], xn.at[pl.ds(0, tokens), cols],
                      core2_send.at[who], core2_recv.at[who], (me_f, other_t))
        side_in = landed(xn.at[pl.ds(0, tokens), cols], core2_send.at[who], core2_recv.at[who])
        if cw % 256 == 0:
            cuts = [(None, span(who * cw, cw // 2)), (None, span(who * cw + cw // 2, cw // 2))]
        else:
            cuts = [(who % 2 == 0, cols), (who % 2 == 1, cols)]
        given = pltpu.make_async_copy(after.at[:, cols], out_ref.at[:, cols], out_sem.at[who])
        giving.append((given, on))
        plans = [(cuts[0], along_chips(who, cuts[0][1])), (cuts[1], across_pair(who, cuts[1][1]))]

        def run():
            @pl.loop(0, 2)
            def _(i):
                at = span(((1 - core) * (1 - i) + core * i) * tokens, tokens)
                part2[at, cols] = jnp.dot(
                    hidden[at, :], wd[who], preferred_element_type=F32).astype(BF16)

                @pl.when(i == 0)
                def _():
                    side.start()
        def join():
            side_in.wait_recv()

            @pl.loop(0, tokens // 128)
            def _(i):
                at = pl.ds(pl.multiple_of(core * tokens + i * 128, 128), 128)
                more = xn[span(i * 128, 128), cols].astype(F32)
                part2[at, cols] = (part2[at, cols].astype(F32) + more).astype(BF16)
            for (this, _), (first, _, _, _) in plans:
                def begin():
                    for out, _ in first:
                        out.start()
                when(this, begin)

        def middle():
            for (this, _), (first, second, add, _) in plans:
                def pass_on():
                    for _, back in first:
                        back.wait_recv()
                    add()
                    for out, _ in second:
                        out.start()
                when(this, pass_on)

        def end():
            for (this, cut), (first, second, _, rest) in plans:
                def close():
                    for _, back in second:
                        back.wait_recv()
                    total = part2[mine, cut].astype(F32) + rest()
                    after[:, cut] = (after[:, cut].astype(F32) + total).astype(BF16)
                    for out, _ in first + second:
                        out.wait_send()
                when(this, close)
            given.start()
            side.wait_send()

        when(on, run)
        joins.append((join, on))
        middles.append((middle, on))
        finals.append((end, on))
        n = len(middles) - 1
        if all_fold:
            for role, plan in ((inner, inner_plan), (is_end, end_plan)):
                for kind, k in plan.get(n, ()):
                    follow(kind, k, role)
        else:
            follow(joins, n)
            if n >= 2:
                follow(middles, n - 2)

    if all_fold:
        inner_order = [[(0, False), (1, False), (0, True), (1, True)],
                       [(2, False), (3, False), (2, True), (3, True)], [(4, False), (5, False)],
                       [(4, True), (5, True)], [(6, True), (6, False)]]
        end_order = [[(0, False), (1, False), (0, True), (1, True), (2, False), (3, False)],
                     [(2, True), (3, True), (4, False)], [(5, False), (4, True), (5, True), (6, True), (6, False)]]
    else:
        by_round = [(n, out) for n in range(per) for out in (False, True)]
        inner_order = [[], [], [], [], by_round]
        end_order = [[], [], by_round]

    def arrivals(part):
        for n, out in part:
            arrive(n, out)

    def inner_front():
        send(0, out=True)
        send(1, out=True)
        line_send_round(0, out=True)

        when(None if all_fold else folds, aside[0].start)
        line_send_round(per_line, out=True)
        when(None if all_fold else folds, aside[1].start)
        for copy in loads:
            copy.wait()
        send_in(0)
        send_in(1)
        for copy in row_loads:
            copy.wait()
        norm_into(xn, tokens + me_t * rows, resid_ref, mix_gain_ref)
        tok_start(own_set)
        for copy in own[1:]:
            copy.start()
        hooks = {(0, 1, 0): mate_tokens(0), (0, 1, 1): lambda: tok_pass(own_set),
                 (1, 0, 0): mate_tokens(1), (1, 0, 2): mate_pass(0), (1, 1, 0): mate_pass(1)}
        order = list(hooks)

        def drain(upto):
            while order and order[0] <= upto:
                hooks[order.pop(0)]()

        for head in range(heads):
            last = head == heads - 1
            first = 2 * head * per_in
            for n in range(per_in):
                arrive_in(first + n)
                drain((head, 0, n))
                if n == 1:
                    if last:
                        send(0, out=False)
                        send(1, out=False)

                    def pushed():
                        puts_in[head].wait_recv()
                    when(None if all_fold else folds, pushed)
                    send_in(first + per_in)
                    send_in(first + per_in + 1)
            for n in range(per_in):
                arrive_in(first + per_in + n)
                if n == 0:
                    if last:
                        for g in range(2):
                            swaps[g].start()
                        arrivals(inner_order[0])
                    else:
                        send_in(first + 2 * per_in)
                        send_in(first + 2 * per_in + 1)
                drain((head, 1, n))
                if n == 0 and last:
                    drain((2, 0, 0))
                    for part in range(2):
                        when(None if all_fold else folds, lambda: tok_wait(mate_sets[part]))
                    for early in range(head):
                        mate_heads(early)
            if not last:
                if head == 0:
                    tok_wait(own_set)
                heads_of(1, head)
        if heads == 1:
            tok_wait(own_set)
        mate_heads(heads - 1)
        arrivals(inner_order[1])
        arrivals(inner_order[2])
        line_send_round(0, out=False)
        heads_of(1, heads - 1)
        arrivals(inner_order[3])
        swaps_in[0].wait_recv()
        line_send_round(1)
        arrivals(inner_order[4])

    def end_front():
        send(0, out=True)
        send(1, out=True)
        for g in range(2):
            swaps[g].start()
        for copy in loads:
            copy.wait()
        puts[0].start()
        for copy in row_loads:
            copy.wait()
        norm_into(xn, me_t * rows, resid_ref, mix_gain_ref)
        for out, _ in to_mate:
            out.start()
        for head in range(1, heads):
            puts[head].start()
        send(0, out=False)
        send(1, out=False)
        for copy in own[1:]:
            copy.start()
        arrivals(end_order[0])
        swaps_in[0].wait_recv()
        aside_in[0].wait_recv()
        across_end[0].start()
        line_send_round(0)
        arrivals(end_order[1])
        line_send_round(1)
        aside_in[1].wait_recv()
        across_end[1].start()
        line_send_round(per_line)
        swaps_in[1].wait_recv()
        line_send_round(per_line + 1)
        arrivals(end_order[2])
        for back in gates_in:
            back.wait_recv()

    pl.when(inner)(inner_front)
    pl.when(is_end)(end_front)
    own[1].wait()
    mix_out()
    line_arrive(0, False)
    line_arrive(1, False)

    def inner_down():
        line_send_round(per_line, out=False)
        swaps_in[1].wait_recv()
        line_send_round(per_line + 1)
    pl.when(inner)(inner_down)

    line_arrive(0, True)
    for copy, on in xn_sends:
        pl.when(on)(copy.wait_send)
    for c in range(chunks):
        mix_chunk(c)
        if c == 3:
            line_arrive(1, True)
        if c > 1:
            take_pair(c - 2)
    line_arrive(2, False)
    line_arrive(3, False)
    line_arrive(2, True)
    for c in range(chunks - 2, chunks):
        take_pair(c)
    for c in range(chunks // 2):
        if c == chunks // 4:
            line_arrive(3, True)
        take_chip(c)
    for k in range(4, per_line):
        line_arrive(k, False)
        line_arrive(k, True)
    for k in range(2):
        line_arrive(per_line + k, False)

    def end_landed():
        for back in across_in:
            back.wait_recv()
    pl.when(is_end)(end_landed)
    own[2].wait()
    own[3].wait()
    take_core(to_core)
    take_core(pair_core)
    for c in range(chunks // 2, chunks):
        take_chip(c)
        take_corner(c - chunks // 2)
        if c == chunks // 2:
            lift(chip, pair, (0, 1))
        elif c == chunks // 2 + 1:
            lift(chip, 1 - pair, (0, 1))
    line_arrive(per_line, True)
    others = [(chip + e) % chips for e in range(1, chips)]
    for x in others:
        lift(x, pair, (core,))
    for c in range(chunks // 2, chunks - 2):
        take_corner(c)
    take_core(chip_core)
    for x in others:
        lift(x, pair, (1 - core,))
    for c in range(chunks - 2, chunks):
        take_corner(c)
    for x in others:
        lift(x, 1 - pair, (core,))
    take_core(corner_core)
    for x in others:
        lift(x, 1 - pair, (1 - core,))
    line_arrive(per_line + 1, True)
    inward = range(1, lines // 2)
    blocks = [None, None]
    for dist in range(1, lines):
        first = per_line + 2 * (dist - 1)
        for out in (True, False):
            if out or dist in inward:
                blocks += [(first, out), (first + 1, out)]
    for n, this in enumerate(blocks):
        if this is None:
            lower(me_f if n == 0 else other_f)
            continue
        m, out = this
        _, dist, turn = line_rounds[m]
        if all_fold:
            if n == 2:
                pl.when(inner)(lambda: line_arrive(per_line + 2, True))
            elif n == 5:
                pl.when(inner)(lambda: line_arrive(per_line + 3, True))
            if dist == 2:
                pl.when(is_end)(lambda: line_arrive(m, True))
            elif dist > 2:
                line_arrive(m, True)
        elif dist > 1:
            line_arrive(m, out)
        at = line + dist - 2 * dist * upper if out else line - dist + 2 * dist * upper
        has = jnp.logical_and(at >= 0, at <= lines - 1)
        if not out:
            has = jnp.logical_and(has, at // (lines // 2) == upper)
        lower(2 * at + (pair if turn == 0 else 1 - pair), has)

    for copy, on in started:
        when(on, copy.wait_send)
    early = 2 + 4 * (lines // 2 - 1) if all_fold else 0
    for end, on in finals[:early]:
        when(on, end)
    if all_fold:
        for role, plan in ((inner, inner_plan), (is_end, end_plan)):
            for kind, k in plan[None]:
                follow(kind, k, role)
    else:
        for n in range(len(middles) - 2, len(middles)):
            follow(middles, n)
    for end, on in finals[early:]:
        when(on, end)
    for given, on in giving:
        when(on, given.wait)


def on_device(fs, tp, resid, mix_gain, w_query, w_key, w_value, w_gate, w_output, decay_rate,
              mlp_gain, w_up, w_down):
    rows, width = resid.shape
    tokens = rows * tp
    in_width = w_query.shape[1] + w_key.shape[1] + w_value.shape[1] + w_gate.shape[1]
    chips = tp // 2
    heads = decay_rate.shape[0]
    wide = CHUNKS * (3 + 4 * (chips - 1))
    hbm = pl.BlockSpec(memory_space=pl.ANY)
    dma = pltpu.SemaphoreType.DMA
    cols = width // fs
    return pl.pallas_call(
        functools.partial(kernel, fs, tp),
        out_shape=jax.ShapeDtypeStruct((rows, width), BF16),
        in_specs=[hbm] * 3 + [pl.BlockSpec(memory_space=pltpu.SMEM)] + [hbm] * 7,
        out_specs=hbm,
        scratch_shapes=[
            pltpu.VMEM((rows, width), BF16),
            pltpu.VMEM((1, width), F32),
            pltpu.VMEM((1, width), F32),
            dma((3,)),
            dma((fs,)),
            pltpu.VMEM((heads, width, in_width // heads), BF16),
            pltpu.VMEM((fs, w_output.shape[0], cols), BF16),
            pltpu.VMEM((width, w_up.shape[1] // 2), BF16),
            pltpu.VMEM((fs, w_down.shape[0] // 2, cols), BF16),
            pltpu.VMEM((2 * tokens, width), BF16),
            pltpu.VMEM((2 * tokens, width), BF16),
            pltpu.VMEM((tokens, in_width // heads), BF16),
            pltpu.VMEM((2, tokens, w_output.shape[0]), BF16),
            pltpu.VMEM((2 * tokens, w_up.shape[1] // 2), BF16),
            pltpu.VMEM((tokens, width), BF16),
            pltpu.VMEM((chips, rows, width), BF16),
            pltpu.VMEM((chips - 1, rows, width), BF16),
            pltpu.VMEM((2 * tokens, width), BF16),
            pltpu.VMEM((2 * chips - 1, rows, width), BF16),
            pltpu.VMEM((rows, width), BF16),
            dma((2, fs - 1)),
            dma((2, fs - 1)),
            dma((3,)),
            dma((4 * heads,)),
            dma((2, 2 * heads * (fs - 5))),
            dma((2, 2 * heads * (fs - 5))),
            dma((heads,)),
            dma((heads,)),
            dma((3 * (2 * chips - 1) + 2,)),
            dma((3 * (2 * chips - 1) + 2,)),
            dma((heads,)),
            dma((heads,)),
            dma((2,)),
            dma((2,)),
            dma((2,)),
            dma((2,)),
            dma((2, 2 * (fs - 2))),
            dma((2, 2 * (fs - 2))),
            dma((2,)),
            dma((2,)),
            dma((2 * chips,)),
            dma((2 * chips,)),
            dma((CHUNKS * (chips - 1),)),
            dma((CHUNKS * (chips - 1),)),
            dma((wide,)),
            dma((wide,)),
            dma((fs,)),
            dma((fs,)),
            dma((2 * (2 * chips - 1), fs)),
            dma((2 * (2 * chips - 1), fs)),
        ],
        compiler_params=pltpu.CompilerParams(
            collective_id=0, has_side_effects=True, vmem_limit_bytes=67043328),
    )(resid, mix_gain[None, :], mlp_gain[None, :], decay_rate, w_query, w_key, w_value,
      w_gate, w_output, w_up, w_down)


def solution(mesh):
    placed = (
        P(("fs", "tp"), None),
        P(),
        P("fs", "tp"),
        P("fs", "tp"),
        P("fs", "tp"),
        P("fs", "tp"),
        P("tp", "fs"),
        P("tp"),
        P(),
        P("fs", "tp"),
        P("tp", "fs"),
    )
    sizes = dict(mesh.shape)
    return jax.shard_map(
        functools.partial(on_device, sizes["fs"], sizes["tp"]), mesh=mesh, in_specs=placed,
        out_specs=P(("fs", "tp"), None), check_vma=False)
```
